32 devices in a mesh: ep: 4 (over y, x), tp: 8 (over z, core).
Axes of the slice: x: 2, y: 2, z: 4, core: 2. Of those that a mesh axis runs over, the one named last changes fastest.
Arguments:
- query_heads_rows: bfloat16 [2048, 2048], P('ep', 'tp'), may hold values from -9 to 9
- key_heads_rows: bfloat16 [2048, 2048], P('ep', 'tp'), may hold values from -9 to 9
- value_heads_rows: bfloat16 [2048, 2048], P('ep', 'tp'), may hold values from -6 to 6
- write_strength_logit: bfloat16 [16, 2048], P('tp', 'ep'), may hold values from -3.5 to -1
- decay_preactivation: bfloat16 [16, 2048], P('tp', 'ep'), may hold values from -5 to 5
- head_decay_logarithm: float32 [16], P('tp'), may hold values from -20 to -3
- extra_log_decay: float32 [16, 2048], P('tp', 'ep'), may hold values from -0.7 to 0
- output_weight: bfloat16 [2048, 2048], P('tp'), may hold values from -2 to 2
- second_batch_tokens: bfloat16 [4096, 2048], P(('ep', 'tp')), may hold values from -6 to 6
- expert_norm_scale: float32 [2048], replicated, may hold values from 0.1 to 1.9
- expert_choice_index: int32 [4096, 2], P(('ep', 'tp')), may hold values from 0 to 15, as said below
- group_router_weight: float32 [4096], P(('ep', 'tp')), may hold values from 0.25 to 1
- expert_logit_difference: float32 [4096], P(('ep', 'tp')), may hold values from -8 to 8
- expert_gate_weight: bfloat16 [16, 1024, 2048], P('ep', 'tp'), may hold values from -0.125 to 0.125
- expert_up_weight: bfloat16 [16, 1024, 2048], P('ep', 'tp'), may hold values from -0.125 to 0.125
- expert_down_weight: bfloat16 [16, 1024, 2048], P('ep', 'tp'), may hold values from -0.375 to 0.375
Outputs:
- mixer_output_first: bfloat16 [2048, 2048], P(('ep', 'tp'))
- expert_out: bfloat16 [4096, 2048], P(('ep', 'tp'))
The draws below stay inside these ranges and needn't reach their ends.
Inputs may be any that keep to these rules, and one draw needn't show every extreme that they name: `expert_choice_index`: each row names two different experts of one group, the experts a * 4 to a * 4 + 3 for some a. In the rows of one device (aligned blocks of 128 rows) no expert is named more than 32 times, and in every device's rows some expert is named exactly 32 times.
All inputs are finite; a program needn't handle non-finite values.
Results may differ from the reference program's by a relative error of at most 0.018.
Values may be sent and summed in bfloat16 or wider, within the bound.
A program may use at most 128 MiB of HBM per device.

```python
import jax
import jax.numpy as jnp
from jax import lax

D = 2048
HEADS = 16
DK = 128
DV = 128
BLOCK = 64
TOK_AEP = 512
SEQ = 2048
TOK_B = 128
CAP = 32
TOKENS_B = 4096
FF = 1024
EXPERTS = 16
GROUPS = 4
EPG = 4
TOPK = 2


def shared_directions(key):
    return jax.random.truncated_normal(jax.random.fold_in(key, 71), -3.0, 3.0, (HEADS, DK))


def coherent_rows(key, salt, lowest, highest):
    level_key, noise_key = jax.random.split(jax.random.fold_in(key, salt))
    direction = shared_directions(key)
    noise = jax.random.truncated_normal(noise_key, -3.0, 3.0, (SEQ, HEADS, DK))
    levels = jax.random.uniform(level_key, (SEQ // BLOCK, HEADS), minval=lowest, maxval=highest)
    per_position = jnp.repeat(levels, BLOCK, axis=0)
    rows = per_position[:, :, None] * direction[None, :, :] + noise
    return rows.reshape(SEQ, HEADS * DK).astype(jnp.bfloat16)


def draw_query_heads_rows(key, part):
    return coherent_rows(key, 13, 0.8, 1.2)


def draw_key_heads_rows(key, part):
    return coherent_rows(key, 12, 1.2, 1.8)


def draw_head_decay_logarithm(key, part):
    pick_key, slow_key, fast_key = jax.random.split(key, 3)
    slow_share = 0.5
    chosen = jax.random.uniform(pick_key, (HEADS,)) < slow_share
    slow_rate = jnp.log(jnp.log(10.0) / (2.4 * SEQ)) + jax.random.uniform(slow_key, (HEADS,), minval=-0.3, maxval=0.3)
    fast_rate = jnp.log(1.0 / 32.0) + jax.random.uniform(fast_key, (HEADS,), minval=-0.3, maxval=0.3)
    return jnp.where(chosen, slow_rate, fast_rate).astype(jnp.float32)


def draw_decay_preactivation(key, part):
    jitter_key, device_key, block_key, run_key = jax.random.split(key, 4)
    segments_count = SEQ // TOK_AEP
    jitter = 0.5 * jax.random.truncated_normal(jitter_key, -3.0, 3.0, (HEADS, SEQ))
    per_device = jax.random.uniform(device_key, (segments_count,), minval=-1.5, maxval=1.5)
    run_start = jax.random.randint(run_key, (), 0, max(segments_count - 2, 1))
    segment_index = jnp.arange(segments_count, dtype=jnp.int32)
    in_run = (segment_index >= run_start) & (segment_index < run_start + 3)
    per_device = jnp.where(in_run, -3.0, per_device)
    per_block = jax.random.uniform(block_key, (SEQ // BLOCK,), minval=-0.5, maxval=0.5)
    offsets = jnp.repeat(per_device, TOK_AEP) + jnp.repeat(per_block, BLOCK)
    return jnp.clip(jitter + offsets[None, :], -5.0, 5.0).astype(jnp.bfloat16)


def draw_extra_log_decay(key, part):
    place_key, depth_key = jax.random.split(key)
    half_length = SEQ // 2
    places = jax.random.randint(place_key, (HEADS, 2), 0, half_length) + jnp.array([0, half_length], jnp.int32)[None, :]
    depths = jnp.log(jax.random.uniform(depth_key, (HEADS, 2), minval=0.5, maxval=0.8))
    positions = jnp.arange(SEQ, dtype=jnp.int32)
    markers = (positions[None, None, :] == places[:, :, None]).astype(jnp.float32)
    return jnp.sum(markers * depths[:, :, None], axis=1).astype(jnp.float32)


def route_block(block_key):
    hot_key, split_key, order_key = jax.random.split(block_key, 3)
    hot_rows = EPG * CAP // 2
    hot_group = jax.random.randint(hot_key, (), 0, GROUPS)
    remain = jnp.asarray(TOK_B - hot_rows, jnp.int32)
    split_keys = jax.random.split(split_key, GROUPS - 1)
    others = []
    for number in range(GROUPS - 2):
        lowest = jnp.maximum(0, remain - hot_rows * (GROUPS - 2 - number))
        highest = jnp.minimum(hot_rows, remain)
        counted = jax.random.randint(split_keys[number], (), lowest, highest + 1).astype(jnp.int32)
        others.append(counted)
        remain = remain - counted
    others.append(remain)
    other_counts = jnp.stack(others).astype(jnp.int32)
    group_index = jnp.arange(GROUPS, dtype=jnp.int32)
    shifted = jnp.clip(group_index - (group_index > hot_group).astype(jnp.int32), 0, GROUPS - 2)
    counts = jnp.where(group_index == hot_group, hot_rows, other_counts[shifted]).astype(jnp.int32)
    group_ends = jnp.cumsum(counts)
    starts = group_ends - counts
    places = jax.random.permutation(order_key, TOK_B).astype(jnp.int32)
    groups = jnp.sum((places[:, None] >= group_ends[None, :]).astype(jnp.int32), axis=1)
    within = places - starts[groups]
    first_id = groups * EPG + within % EPG
    second = groups * EPG + (within + 1 + within // EPG % (EPG - 1)) % EPG
    return jnp.stack([first_id, second], axis=1).astype(jnp.int32)


def draw_expert_choice_index(key, part):
    block_keys = jax.random.split(key, TOKENS_B // TOK_B)
    return jax.vmap(route_block)(block_keys).reshape(TOKENS_B, TOPK).astype(jnp.int32)


def shard_levels(rng, shape, cuts, smallest, top_value):
    loudness, own = 1.0, jax.random.fold_in(rng, 6)
    for dim, blocks in cuts:
        draws = jnp.exp(jax.random.uniform(jax.random.fold_in(own, dim), (blocks,), jnp.float32, smallest / len(cuts), top_value / len(cuts)))
        loudness = loudness * jnp.repeat(draws, shape[dim] // blocks).reshape([-1 if axis == dim else 1 for axis in range(len(shape))])
    return loudness


def normal_values(own_key, extent, deviation, bound, cuts=(), kind=jnp.bfloat16):
    factor_of = shard_levels(own_key, extent, cuts, -0.22, 0.18) if cuts else 1.0
    drawn = jax.random.normal(own_key, extent, jnp.float32) * deviation * factor_of
    return jnp.minimum(jnp.maximum(drawn, -bound), bound).astype(kind)


def setup_inputs(seed: int = 0) -> dict:
    key_of = jax.random.split(jax.random.key(seed), 17)
    query_heads_rows = draw_query_heads_rows(jax.random.fold_in(key_of[16], 71), 0)
    key_heads_rows = draw_key_heads_rows(jax.random.fold_in(key_of[16], 71), 0)
    value_heads_rows = normal_values(key_of[2], (SEQ, HEADS * DV), 1.0, 6.0, ((0, 4), (1, 8)))
    write_strength_logit = jnp.clip(-3.5 + 2.5 * jax.random.uniform(key_of[3], (HEADS, SEQ), jnp.float32) ** shard_levels(key_of[3], (HEADS, SEQ), ((0, 8), (1, 4)), -0.2, 0.2), -3.5, -1.0).astype(jnp.bfloat16)
    decay_preactivation = draw_decay_preactivation(jax.random.fold_in(key_of[16], 71), 0)
    head_decay_logarithm = draw_head_decay_logarithm(jax.random.fold_in(key_of[16], 71), 0)
    extra_log_decay = draw_extra_log_decay(jax.random.fold_in(key_of[16], 71), 0)
    output_weight = normal_values(key_of[7], (HEADS * DV, D), ((HEADS * DV) // 256) ** -0.5, 2.0, ((0, 8),))
    second_batch_tokens = normal_values(key_of[8], (TOKENS_B, D), 1.0, 6.0, ((0, 32),))
    expert_norm_scale = jnp.clip(1.0 + 0.18 * jax.random.normal(key_of[9], (D,), jnp.float32), 0.1, 1.9)
    expert_choice_index = draw_expert_choice_index(jax.random.fold_in(key_of[16], 71), 0)
    group_router_weight = jnp.clip(0.25 + 0.75 * jax.random.uniform(key_of[11], (TOKENS_B,), jnp.float32) ** shard_levels(key_of[11], (TOKENS_B,), ((0, 32),), -0.2, 0.2), 0.25, 1.0)
    expert_logit_difference = normal_values(key_of[12], (TOKENS_B,), 1.5, 8.0, ((0, 32),), jnp.float32)
    expert_gate_weight = normal_values(key_of[13], (EXPERTS, FF, D), D ** -0.5, 0.125, ((0, 4), (1, 8)))
    expert_up_weight = normal_values(key_of[14], (EXPERTS, FF, D), D ** -0.5, 0.125, ((0, 4), (1, 8)))
    expert_down_weight = normal_values(key_of[15], (EXPERTS, FF, D), (FF // 4) ** -0.5, 0.375, ((0, 4), (1, 8)))
    return dict(query_heads_rows=query_heads_rows, key_heads_rows=key_heads_rows, value_heads_rows=value_heads_rows, write_strength_logit=write_strength_logit, decay_preactivation=decay_preactivation, head_decay_logarithm=head_decay_logarithm, extra_log_decay=extra_log_decay, output_weight=output_weight, second_batch_tokens=second_batch_tokens, expert_norm_scale=expert_norm_scale, expert_choice_index=expert_choice_index, group_router_weight=group_router_weight, expert_logit_difference=expert_logit_difference, expert_gate_weight=expert_gate_weight, expert_up_weight=expert_up_weight, expert_down_weight=expert_down_weight)


precise_setting = lax.Precision.HIGHEST
norm_eps = 1e-06

def unit_rows(matrix):
    return matrix * lax.rsqrt(lax.optimization_barrier(jnp.sum(matrix * matrix, axis=-1, keepdims=True)) + norm_eps)

def block_terms(query_block, key_block, value_block, decay_logarithm, strength):
    span_len = query_block.shape[2]
    dim_value = value_block.shape[-1]
    cumulative = jnp.cumsum(decay_logarithm, axis=-1)
    within = jnp.tril(jnp.ones((span_len, span_len), bool))
    strict = jnp.tril(jnp.ones((span_len, span_len), bool), -1)
    spread = cumulative[..., :, None] - cumulative[..., None, :]
    decayed = jnp.where(within, jnp.exp(jnp.where(within, spread, 0.0)), 0.0)
    weighted = key_block * strength[..., None]
    lower_part = jnp.where(strict, jnp.einsum('hnid,hnjd->hnij', weighted, key_block, precision=precise_setting) * decayed, 0.0)
    system = lower_part + jnp.eye(span_len, dtype=jnp.float32)
    rhs_cols = jnp.concatenate([value_block * strength[..., None], weighted * jnp.exp(cumulative)[..., None]], axis=-1)
    solved = jax.scipy.linalg.solve_triangular(system, rhs_cols, lower=True, unit_diagonal=True)
    updated_values = solved[..., :dim_value]
    delta_corrections = solved[..., dim_value:]
    scores = jnp.where(within, jnp.einsum('hnid,hnjd->hnij', query_block, key_block, precision=precise_setting) * decayed, 0.0)
    decayed_queries = query_block * jnp.exp(cumulative)[..., None]
    decayed_keys = key_block * jnp.exp(cumulative[..., -1:] - cumulative)[..., None]
    block_retention = jnp.exp(cumulative[..., -1])
    return (decayed_queries, decayed_keys, updated_values, delta_corrections, scores, block_retention)

def carry_step(recurrent_state, inputs):
    decayed_queries, decayed_keys, updated_values, delta_corrections, scores, block_retention = inputs
    value_updates = updated_values - jnp.einsum('jdb,jbu->jdu', delta_corrections, recurrent_state, precision=precise_setting)
    final_output = jnp.einsum('jdb,jbu->jdu', decayed_queries, recurrent_state, precision=precise_setting)
    final_output = final_output + jnp.einsum('hcj,hjv->hcv', scores, value_updates, precision=precise_setting)
    recurrent_state = recurrent_state * block_retention[:, None, None] + jnp.einsum('rpq,rpd->rqd', decayed_keys, value_updates, precision=precise_setting)
    return (recurrent_state, final_output)

def mixer_portion(query_heads_rows, key_heads_rows, value_heads_rows, write_strength_logit, decay_preactivation, head_decay_logarithm, extra_log_decay, output_weight):
    length = query_heads_rows.shape[0]
    blocks = length // BLOCK

    def heads_first(matrix):
        spread_out = matrix.astype(jnp.float32).reshape(length, HEADS, -1).transpose(1, 0, 2)
        return spread_out.reshape(HEADS, blocks, BLOCK, -1)
    query_block = unit_rows(heads_first(query_heads_rows)) * DK ** (-0.5)
    key_block = unit_rows(heads_first(key_heads_rows))
    value_block = heads_first(value_heads_rows)
    strength = jax.nn.sigmoid(write_strength_logit.astype(jnp.float32)).reshape(HEADS, blocks, BLOCK)
    decay_logarithm = -jnp.exp(head_decay_logarithm)[:, None] * jax.nn.softplus(decay_preactivation.astype(jnp.float32)) + extra_log_decay
    decay_logarithm = decay_logarithm.reshape(HEADS, blocks, BLOCK)
    terms = block_terms(query_block, key_block, value_block, decay_logarithm, strength)
    inputs = tuple((jnp.moveaxis(term, 1, 0) for term in terms))
    _, outputs = lax.scan(carry_step, jnp.zeros((HEADS, DK, DV), jnp.float32), inputs)
    attention_result = outputs.transpose(0, 2, 1, 3).reshape(length, HEADS * DV).astype(jnp.bfloat16)
    return jnp.dot(attention_result.astype(jnp.float32), output_weight.astype(jnp.float32), preferred_element_type=jnp.float32).astype(jnp.bfloat16)

def experts_part(second_batch_tokens, expert_norm_scale, expert_choice_index, group_router_weight, expert_logit_difference, expert_gate_weight, expert_up_weight, expert_down_weight):
    widened = second_batch_tokens.astype(jnp.float32)
    normed = (widened * lax.rsqrt(lax.optimization_barrier(jnp.mean(widened * widened, axis=-1, keepdims=True)) + norm_eps) * expert_norm_scale).astype(jnp.bfloat16)
    token_count = second_batch_tokens.shape[0]
    width_model = second_batch_tokens.shape[1]
    flat_ids = expert_choice_index.reshape(-1).astype(jnp.int32)
    copy_count = flat_ids.shape[0]
    sorted_order = jnp.argsort(flat_ids, stable=True).astype(jnp.int32)
    sorted_ids = flat_ids[sorted_order]
    counts = lax.optimization_barrier(jnp.sum((flat_ids[:, None] == jnp.arange(EXPERTS, dtype=jnp.int32)[None, :]).astype(jnp.int32), axis=0))
    starts = jnp.cumsum(counts) - counts
    padded = (counts + 127) // 128 * 128
    pad_ends = jnp.cumsum(padded)
    pad_starts = pad_ends - padded
    destination = (pad_starts[sorted_ids] + jnp.arange(copy_count, dtype=jnp.int32) - starts[sorted_ids]).astype(jnp.int32)
    segments = -(-copy_count // 128) + EXPERTS
    source = jnp.full((segments * 128,), token_count, jnp.int32).at[destination].set((sorted_order // TOPK).astype(jnp.int32))
    padded_rows = jnp.concatenate([normed, jnp.zeros((1, width_model), jnp.bfloat16)], axis=0)
    gathered = padded_rows[source]
    seg_expert = jnp.minimum(jnp.searchsorted(pad_ends, jnp.arange(segments, dtype=jnp.int32) * 128, side='right'), EXPERTS - 1).astype(jnp.int32)

    def one_segment(operands):
        segment_rows, expert = operands
        gating = jnp.dot(segment_rows.astype(jnp.float32), expert_gate_weight[expert].T.astype(jnp.float32), preferred_element_type=jnp.float32)
        upward = jnp.dot(segment_rows.astype(jnp.float32), expert_up_weight[expert].T.astype(jnp.float32), preferred_element_type=jnp.float32)
        hidden = (jax.nn.silu(gating) * upward).astype(jnp.bfloat16)
        return jnp.dot(hidden.astype(jnp.float32), expert_down_weight[expert].astype(jnp.float32), preferred_element_type=jnp.float32).astype(jnp.bfloat16)
    results = lax.map(one_segment, (gathered.reshape(segments, 128, width_model), seg_expert))
    per_copy = results.reshape(-1, width_model)[destination]
    unsorted = jnp.zeros((copy_count, width_model), jnp.bfloat16).at[sorted_order].set(per_copy)
    copies = unsorted.reshape(token_count, TOPK, width_model).astype(jnp.float32)
    leading = jax.nn.sigmoid(expert_logit_difference)
    weights = group_router_weight[:, None] * jnp.stack([leading, 1.0 - leading], axis=-1)
    return lax.optimization_barrier(jnp.sum(weights[..., None] * copies, axis=1)).astype(jnp.bfloat16)

def reference(query_heads_rows, key_heads_rows, value_heads_rows, write_strength_logit, decay_preactivation, head_decay_logarithm, extra_log_decay, output_weight, second_batch_tokens, expert_norm_scale, expert_choice_index, group_router_weight, expert_logit_difference, expert_gate_weight, expert_up_weight, expert_down_weight):
    mixer_output_first = mixer_portion(query_heads_rows, key_heads_rows, value_heads_rows, write_strength_logit, decay_preactivation, head_decay_logarithm, extra_log_decay, output_weight)
    expert_out = experts_part(second_batch_tokens, expert_norm_scale, expert_choice_index, group_router_weight, expert_logit_difference, expert_gate_weight, expert_up_weight, expert_down_weight)
    return (mixer_output_first, expert_out)
```

```python
import functools

import jax
import jax.numpy as jnp
from jax import lax
from jax.experimental import pallas as pl
from jax.experimental.pallas import tpu as pltpu
from jax.sharding import PartitionSpec as P

DK = 128
DV = 128
CAP = 32
RING = 4
MESH = pl.DeviceIdType.MESH
EPG = 4
TOPK = 2


precise_setting = lax.Precision.HIGHEST
norm_eps = 1e-06


def incoming(end_memory, axis):
    count, mine = (lax.axis_size(axis), lax.axis_index(axis))
    pieces = lax.all_gather(end_memory, axis)
    state = jnp.zeros(end_memory.shape[:-1] + (DV,), jnp.float32)
    for position in range(count - 1):
        end, transfer = pieces[position, ..., :DV], pieces[position, ..., DV:]
        longer = end + jnp.einsum("hij,hjv->hiv", transfer, state, precision=precise_setting)
        state = jnp.where(position < mine, longer, state)
    return state


def unit_rows(matrix):
    return matrix * lax.rsqrt(jnp.sum(matrix * matrix, axis=-1, keepdims=True) + norm_eps)


def mm(a, b, dims=((1,), (0,))):
    return lax.dot_general(
        a, b, (dims, ((), ())), precision=precise_setting, preferred_element_type=jnp.float32
    )


def delta_body(q_ref, k_ref, v_ref, strength_ref, decay_ref, local_ref, proj_ref, end_ref):
    heads = strength_ref.shape[0]
    chunk = DK
    chunks = q_ref.shape[0] // chunk
    rows = lax.broadcasted_iota(jnp.int32, (chunk, chunk), 0)
    cols = lax.broadcasted_iota(jnp.int32, (chunk, chunk), 1)
    within = rows >= cols
    eye = jnp.where(rows == cols, 1.0, 0.0)
    parts = []
    for h in range(heads):
        for c in range(chunks):
            at = pl.ds(c * chunk, chunk)
            q = q_ref[at, h * DK : (h + 1) * DK].astype(jnp.float32)
            k = k_ref[at, h * DK : (h + 1) * DK].astype(jnp.float32)
            v = v_ref[at, h * DV : (h + 1) * DV].astype(jnp.float32)
            q = unit_rows(q) * DK ** (-0.5)
            k = unit_rows(k)
            d_row = decay_ref[h : h + 1, c * chunk : (c + 1) * chunk]
            b_row = strength_ref[h : h + 1, c * chunk : (c + 1) * chunk]
            d_col = jnp.sum(jnp.where(rows == cols, d_row, 0.0), axis=1, keepdims=True)
            b_col = jnp.sum(jnp.where(rows == cols, b_row, 0.0), axis=1, keepdims=True)
            cum_col = jnp.sum(jnp.where(within, d_row, 0.0), axis=1, keepdims=True)
            cum_row = jnp.sum(jnp.where(rows <= cols, d_col, 0.0), axis=0, keepdims=True)
            last = cum_col[chunk - 1 : chunk, :]
            decayed = jnp.where(within, jnp.exp(jnp.where(within, cum_col - cum_row, 0.0)), 0.0)
            weighted = k * b_col
            lower = jnp.where(
                rows > cols, mm(weighted, k, ((1,), (1,))) * decayed, 0.0
            )
            scores = mm(q, k, ((1,), (1,))) * decayed
            grown = jnp.exp(cum_col)
            rhs = jnp.concatenate([v * b_col, weighted * grown], axis=1)
            parts.append([lower, scores, rhs, q * grown, k * jnp.exp(last - cum_col), jnp.exp(last)])
    inverses = [None] * len(parts)
    span = 1
    while span < chunk:
        mask = (
            (rows // (2 * span) == cols // (2 * span))
            & (rows // span % 2 == 1)
            & (cols // span % 2 == 0)
        )
        for i, part in enumerate(parts):
            edge = jnp.where(mask, part[0], 0.0)
            if span == 1:
                inverses[i] = eye - edge
            else:
                inverses[i] = inverses[i] - mm(mm(inverses[i], edge), inverses[i])
        span *= 2
    solved = [mm(inverse, part[2]) for inverse, part in zip(inverses, parts)]
    states = [
        jnp.concatenate([jnp.zeros((DK, DV), jnp.float32), eye], axis=1) for _ in range(heads)
    ]
    for c in range(chunks):
        for h in range(heads):
            _, scores, _, queries, keys, retention = parts[h * chunks + c]
            both = solved[h * chunks + c]
            fresh = jnp.concatenate([both[:, :DV], jnp.zeros((chunk, DK), jnp.float32)], axis=1)
            state = states[h]
            updates = fresh - mm(both[:, DV:], state)
            out = mm(queries, state) + mm(scores, updates)
            states[h] = state * retention + mm(keys, updates, ((0,), (0,)))
            at = pl.ds(c * chunk, chunk)
            local_ref[h, at, :] = out[:, :DV]
            proj_ref[h, at, :] = out[:, DV:]
    for h in range(heads):
        end_ref[h] = states[h].astype(end_ref.dtype)


def delta_rule(queries, keys, values, strength, decay_logarithm):
    heads, length = strength.shape
    vmem = pl.BlockSpec(memory_space=pltpu.VMEM)
    f32 = jnp.float32
    return pl.pallas_call(
        delta_body,
        out_shape=(
            jax.ShapeDtypeStruct((heads, length, DV), f32),
            jax.ShapeDtypeStruct((heads, length, DK), f32),
            jax.ShapeDtypeStruct((heads, DK, DV + DK), f32),
        ),
        in_specs=[vmem] * 5,
        out_specs=(vmem,) * 3,
        cost_estimate=pl.CostEstimate(
            flops=40 * heads * length * DK * DK * 6, bytes_accessed=4 * 2**20, transcendentals=0
        ),
        compiler_params=pltpu.CompilerParams(vmem_limit_bytes=40 * 2**20),
    )(queries, keys, values, strength, decay_logarithm)


def expert_kernel(x_ref, gate_ref, up_ref, down_ref, out_ref):
    experts, units, width = gate_ref.shape
    x = x_ref[:, :width]
    hidden = []
    for e in range(experts):
        gating = lax.dot_general(
            x, gate_ref[e], (((1,), (1,)), ((), ())), preferred_element_type=jnp.float32
        )
        upward = lax.dot_general(
            x, up_ref[e], (((1,), (1,)), ((), ())), preferred_element_type=jnp.float32
        )
        share = x_ref[:, width + e : width + e + 1].astype(jnp.float32) + x_ref[
            :, width + experts + e : width + experts + e + 1
        ].astype(jnp.float32)
        hidden.append((gating / (1.0 + jnp.exp(-gating)) * upward * share).astype(jnp.bfloat16))
    hidden = jnp.concatenate(hidden, axis=1)
    down = down_ref[...].reshape(experts * units, width)
    out_ref[...] = jnp.dot(hidden, down, preferred_element_type=jnp.float32).astype(jnp.bfloat16)


def expert_layer(rows, gate, up, down, tile):
    count, wide = rows.shape
    experts, units, width = gate.shape
    whole = pl.BlockSpec((experts, units, width), lambda i: (0, 0, 0))
    return pl.pallas_call(
        expert_kernel,
        grid=(count // tile,),
        out_shape=jax.ShapeDtypeStruct((count, width), jnp.bfloat16),
        in_specs=[pl.BlockSpec((tile, wide), lambda i: (i, 0)), whole, whole, whole],
        out_specs=pl.BlockSpec((tile, width), lambda i: (i, 0)),
        cost_estimate=pl.CostEstimate(
            flops=6 * count * experts * units * width,
            bytes_accessed=4 * count * width + 6 * experts * units * width,
            transcendentals=0,
        ),
        compiler_params=pltpu.CompilerParams(vmem_limit_bytes=48 * 2**20),
    )(rows, gate, up, down)


def fused_kernel(
    q_hbm, k_hbm, v_hbm, strength_ref, decay_ref, wout_hbm, tokens_hbm, scale_ref, info_ref,
    gate_hbm, up_hbm, down_hbm, mixed_ref, expert_ref,
    q_ref, k_ref, v_ref, wout_ref, tokens_ref, gate_ref, up_ref, down_ref,
    raw, infos, spreads, stage, stage_share, rows, rows_share, hid, res, theirs, back,
    acc, inb, local, proj, attn, states_out, states_in, state, prod, prod_theirs, mixed_in,
    load_sems, ag_s, ag_r, agi_s, agi_r, ep_s, ep_r, eps_s, eps_r, core_s, core_r, cores_s, cores_r,
    pair_s, pair_r, back_s, back_r, rs_s, rs_r, st_s, st_r, pp_s, pp_r, mr_s, mr_r,
):
    e, t = lax.axis_index("ep"), lax.axis_index("tp")
    core, z = lax.rem(t, 2), lax.div(t, 2)
    chips, tokens, width = raw.shape
    peers, slots = stage.shape[1], stage.shape[2]
    experts, units, _ = gate_ref.shape
    count = peers * slots
    halves, half = acc.shape[1], acc.shape[3]
    last = chips - 1
    bf16, f32 = jnp.bfloat16, jnp.float32
    upper = lax.div(z, 2)
    near_end = z + upper * (last - 2 * z)

    def order(i):
        base = (near_end, 1 + 2 * near_end, 2 - 2 * near_end, 3 - near_end)[i]
        return base + upper * (last - 2 * base)

    inner = jnp.logical_and(z >= 1, z <= last - 1)
    outer = jnp.logical_or(z == 0, z == last)
    other = (e, z * 2 + 1 - core)

    def at_chip(chip):
        return (e, chip * 2 + core)

    def at_peer(j):
        return (lax.rem(e + j, peers), t)

    sources = [lax.rem(e + peers - j, peers) for j in range(peers)]

    loads = []
    for i, (src, dst) in enumerate(
        (
            (tokens_hbm, tokens_ref), (q_hbm, q_ref), (k_hbm, k_ref), (v_hbm, v_ref),
            (gate_hbm, gate_ref), (up_hbm, up_ref), (down_hbm, down_ref), (wout_hbm, wout_ref),
        )
    ):
        copy = pltpu.make_async_copy(src, dst, load_sems.at[i])
        copy.start()
        loads.append(copy)

    barrier = pltpu.get_barrier_semaphore()
    greeted = [at_peer(j) for j in range(1, peers)] + [other]
    greeted += [at_chip(lax.rem(z + h, chips)) for h in range(1, chips)]
    for device in greeted:
        pl.semaphore_signal(barrier, inc=1, device_id=device, device_id_type=MESH)

    started = []

    def send(src, dst, send_sem, recv_sem, device, when=None):
        def make():
            return pltpu.make_async_remote_copy(
                src_ref=src, dst_ref=dst, send_sem=send_sem, recv_sem=recv_sem,
                device_id=device, device_id_type=MESH,
            )

        if when is None:
            make().start()
        else:
            @pl.when(when)
            def _():
                make().start()
        started.append((make, when))

    def arrived(dst, send_sem, recv_sem):
        pltpu.make_async_remote_copy(
            src_ref=dst, dst_ref=dst, send_sem=send_sem, recv_sem=recv_sem,
            device_id=other, device_id_type=MESH,
        ).wait_recv()

    loads[0].wait()
    widened = tokens_ref[...].astype(f32)
    raw[z] = (
        widened
        * lax.rsqrt(jnp.mean(widened * widened, axis=-1, keepdims=True) + norm_eps)
        * scale_ref[...]
    ).astype(bf16)
    infos[z] = info_ref[...]
    pl.semaphore_wait(barrier, len(greeted))

    for n, hop in enumerate((2, -2, 1, -1)):
        inside = z <= last - hop if hop > 0 else z >= -hop
        device = at_chip(z + hop)
        send(infos.at[z], infos.at[z], agi_s.at[n], agi_r.at[z], device, inside)
        send(raw.at[z], raw.at[z], ag_s.at[n], ag_r.at[z], device, inside)

    def gathered(i):
        chip = order(i)
        arrived(infos.at[chip], agi_s.at[0], agi_r.at[chip])
        arrived(raw.at[chip], ag_s.at[0], ag_r.at[chip])

    def relay():
        chip = order(1)
        device = at_chip(last * (z - 1))
        send(infos.at[chip], infos.at[chip], agi_s.at[4], agi_r.at[chip], device, inner)
        send(raw.at[chip], raw.at[chip], ag_s.at[4], ag_r.at[chip], device, inner)

    def select(i):
        chip = order(i)
        info = infos[chip]
        goes = info[peers * 8 : peers * 8 + 8]
        before = lax.broadcasted_iota(jnp.int32, (tokens, tokens), 0) < lax.broadcasted_iota(
            jnp.int32, (tokens, tokens), 1
        )
        rank = jnp.dot(
            goes.astype(bf16), jnp.where(before, 1.0, 0.0).astype(bf16), preferred_element_type=f32
        )
        slot = lax.broadcasted_iota(jnp.int32, (tokens, tokens), 0).astype(f32)
        for g in range(peers):
            hit = jnp.logical_and(slot == rank[g : g + 1], goes[g : g + 1] > 0.5)
            spread = jnp.where(hit, 1.0, 0.0)
            share = mm(info[g * 8 : g * 8 + 8], spread, ((1,), (1,)))
            high = share.astype(bf16)
            low = (share - high.astype(f32)).astype(bf16)
            stage_share[chip, g] = jnp.concatenate([high, low], axis=0)
            spreads[chip, g * slots : (g + 1) * slots] = spread[:slots].astype(bf16)

        def columns(n, carry):
            at = pl.ds(pl.multiple_of(n * 512, 512), 512)
            picked = jnp.dot(spreads[chip], raw[chip, :, at], preferred_element_type=f32)
            stage[chip, :, :, at] = picked.astype(bf16).reshape(peers, slots, 512)
            return carry

        lax.fori_loop(0, width // 512, columns, 0)
        for j in (3, 1, 2):
            target = lax.rem(e + j, peers)
            send(
                stage_share.at[chip, target], rows_share.at[chip, core, e],
                eps_s.at[chip, j], eps_r.at[chip, j], (target, t),
            )
            send(
                stage.at[chip, target], rows.at[chip, core, e],
                ep_s.at[chip, j], ep_r.at[chip, j], (target, t),
            )
        rows[chip, core, e] = stage[chip, e]
        rows_share[chip, core, e] = stage_share[chip, e]

    def pass_on(i):
        chip = order(i)
        for j in range(1, peers):
            arrived(rows_share.at[chip, core, sources[j]], eps_s.at[chip, j], eps_r.at[chip, j])
            arrived(rows.at[chip, core, sources[j]], ep_s.at[chip, j], ep_r.at[chip, j])
        send(
            rows_share.at[chip, core], rows_share.at[chip, core],
            cores_s.at[chip], cores_r.at[chip], other,
        )
        send(rows.at[chip, core], rows.at[chip, core], core_s.at[chip], core_r.at[chip], other)

    def produce(i):
        chip = order(i)
        arrived(rows_share.at[chip, 1 - core], cores_s.at[chip], cores_r.at[chip])
        arrived(rows.at[chip, 1 - core], core_s.at[chip], core_r.at[chip])
        unit = lax.broadcasted_iota(jnp.int32, (16, 2 * units), 1) // units
        which = lax.rem(lax.broadcasted_iota(jnp.int32, (16, 2 * units), 0), 8)

        def expert_pair(n, carry):
            pick = jnp.where(which == unit + 2 * n, 1.0, 0.0).astype(bf16)
            share = [
                lax.dot_general(
                    rows_share[chip, c, p], pick, (((0,), (0,)), ((), ())),
                    preferred_element_type=f32,
                )[:slots]
                for c in range(2)
                for p in range(peers)
            ]
            share = jnp.concatenate(share, axis=0)
            x = rows[chip].reshape(2 * count, width)
            gating = lax.dot_general(
                x, gate_ref[pl.ds(2 * n, 2)].reshape(2 * units, width),
                (((1,), (1,)), ((), ())), preferred_element_type=f32,
            )
            upward = lax.dot_general(
                x, up_ref[pl.ds(2 * n, 2)].reshape(2 * units, width),
                (((1,), (1,)), ((), ())), preferred_element_type=f32,
            )
            at = pl.ds(pl.multiple_of(n * 2 * units, 2 * units), 2 * units)
            hid[:, at] = (gating / (1.0 + jnp.exp(-gating)) * upward * share).astype(bf16)
            return carry

        lax.fori_loop(0, experts // 2, expert_pair, 0)

        def columns(n, carry):
            at = pl.ds(pl.multiple_of(n * 512, 512), 512)
            down = down_ref[:, :, at].reshape(experts * units, 512)
            made = jnp.dot(hid[...], down, preferred_element_type=f32)
            res[chip, :, :, :, at] = made.astype(bf16).reshape(2, peers, slots, 512)
            return carry

        lax.fori_loop(0, width // 512, columns, 0)
        send(res.at[chip, 1 - core], theirs.at[chip], pair_s.at[chip], pair_r.at[chip], other)

    def give_back(i):
        chip = order(i)
        arrived(theirs.at[chip], pair_s.at[chip], pair_r.at[chip])
        res[chip, core] = (res[chip, core].astype(f32) + theirs[chip].astype(f32)).astype(bf16)
        for j in (3, 1, 2):
            target = lax.rem(e + j, peers)
            send(
                res.at[chip, core, target], back.at[chip, e],
                back_s.at[chip, j], back_r.at[chip, j], (target, t),
            )
        back[chip, e] = res[chip, core, e]

    def unselect(i):
        chip = order(i)
        for j in range(1, peers):
            arrived(back.at[chip, sources[j]], back_s.at[chip, j], back_r.at[chip, j])
        for h in range(halves):
            acc[chip, h] = lax.dot_general(
                spreads[chip],
                back[chip, :, :, h * half : (h + 1) * half].reshape(count, half),
                (((0,), (0,)), ((), ())), preferred_element_type=f32,
            ).astype(bf16)

    def forward(i, when):
        chip = order(i)
        way = lax.div(z - chip + last, chips)
        follows = (1 - way) * z + way * (last - z) > 0
        following = z + 1 - 2 * way
        ends = way * (1 - lax.min(lax.abs(following - chip), 1))
        slot = chip + ends * (chips - chip)
        for h in range(halves):
            @pl.when(jnp.logical_and(when, follows))
            def _():
                arrived(inb.at[chip, h], rs_s.at[chip, h], rs_r.at[chip, h])
                acc[chip, h] = (acc[chip, h].astype(f32) + inb[chip, h].astype(f32)).astype(bf16)

            send(
                acc.at[chip, h], inb.at[slot, h],
                rs_s.at[chip, h], rs_r.at[slot, h], at_chip(following), when,
            )

    def finish(first, parts, sems, out, at):
        @pl.when(z > 0)
        def _():
            arrived(parts[0], sems[0], sems[1])

        @pl.when(z < last)
        def _():
            arrived(parts[1], sems[0], sems[2])

        @pl.when(z == 0)
        def _():
            out[:, at] = (first[...].astype(f32) + parts[1][...].astype(f32)).astype(bf16)

        @pl.when(z == last)
        def _():
            out[:, at] = (first[...].astype(f32) + parts[0][...].astype(f32)).astype(bf16)

        @pl.when(inner)
        def _():
            total = first[...].astype(f32) + parts[0][...].astype(f32) + parts[1][...].astype(f32)
            out[:, at] = total.astype(bf16)

    heads = strength_ref.shape[0]

    def send_states():
        for j in range(1, peers):
            send(states_out, states_in.at[j], st_s.at[j], st_r.at[j], at_peer(j), e < peers - j)

    def project():
        state[...] = jnp.zeros_like(state)
        for j in range(peers - 1, 0, -1):
            @pl.when(e >= j)
            def _():
                arrived(states_in.at[j], st_s.at[j], st_r.at[j])
                for h in range(heads):
                    piece = states_in[j, h].astype(f32)
                    state[h] = piece[:, :DV] + mm(piece[:, DV:], state[h])
        for h in range(heads):
            attn[:, h * DV : (h + 1) * DV] = (local[h] + mm(proj[h], state[h])).astype(bf16)
        loads[7].wait()
        share = prod.shape[2]

        def columns(n, carry):
            at = pl.ds(pl.multiple_of(n * 512, 512), 512)
            made = jnp.dot(attn[...], wout_ref[:, at], preferred_element_type=f32)
            made = made.astype(bf16).reshape(chips, 2, share, 512)
            for c in range(2):
                prod[c, :, :, at] = made[:, c]
            return carry

        lax.fori_loop(0, width // 512, columns, 0)
        send(prod.at[1 - core], prod_theirs, pp_s, pp_r, other)

    def join_mixed():
        arrived(prod_theirs, pp_s, pp_r)
        prod[core] = (prod[core].astype(f32) + prod_theirs[...].astype(f32)).astype(bf16)

    def mixed_hop(k):
        for way in range(2):
            when = z == (k if way == 0 else last - k)
            targets = range(last, k, -1) if way == 0 else range(0, last - k)
            for chip in targets:
                if k > 0:
                    @pl.when(when)
                    def _():
                        arrived(mixed_in.at[chip], mr_s.at[chip], mr_r.at[chip])
                        prod[core, chip] = (
                            prod[core, chip].astype(f32) + mixed_in[chip].astype(f32)
                        ).astype(bf16)

                ends = way == 1 and last - k - 1 == chip
                slot = chips if ends else chip
                send(
                    prod.at[core, chip], mixed_in.at[slot],
                    mr_s.at[chip], mr_r.at[slot], at_chip(z + 1 - 2 * way), when,
                )

    select(0)
    for i in range(1, 4):
        loads[i].wait()
    delta_body(q_ref, k_ref, v_ref, strength_ref, decay_ref, local, proj, states_out)
    send_states()
    pass_on(0)
    for i in range(4, 7):
        loads[i].wait()
    gathered(1)
    relay()
    select(1)
    produce(0)
    gathered(2)
    select(2)
    project()
    gathered(3)
    select(3)
    join_mixed()
    mixed_hop(0)
    pass_on(1)
    produce(1)
    give_back(1)
    mixed_hop(1)
    pass_on(2)
    produce(2)
    mixed_hop(2)
    pass_on(3)
    produce(3)
    give_back(3)
    give_back(2)
    give_back(0)
    finish(
        prod.at[core, z], (mixed_in.at[z], mixed_in.at[chips]),
        (mr_s.at[0], mr_r.at[z], mr_r.at[chips]), mixed_ref, slice(0, width),
    )
    unselect(1)
    forward(1, outer)
    unselect(3)
    forward(3, outer)
    forward(1, inner)
    unselect(2)
    forward(2, outer)
    forward(3, inner)
    forward(2, inner)
    unselect(0)
    for h in range(halves):
        finish(
            acc.at[z, h], (inb.at[z, h], inb.at[chips, h]),
            (rs_s.at[0, h], rs_r.at[z, h], rs_r.at[chips, h]),
            expert_ref, slice(h * half, (h + 1) * half),
        )
    for make, when in started:
        if when is None:
            make().wait_send()
        else:
            @pl.when(when)
            def _():
                make().wait_send()


def fused(
    queries, keys, values, strength, decay_logarithm, out_weight, tokens, scale, info,
    gate, up, down, slots,
):
    experts, units, width = gate.shape
    count, peers, chips, halves = tokens.shape[0], lax.axis_size("ep"), RING, 2
    heads, length = strength.shape
    half = width // halves
    share = length // (2 * chips)
    bf16, f32 = jnp.bfloat16, jnp.float32
    vmem = pl.BlockSpec(memory_space=pltpu.VMEM)
    anywhere = pl.BlockSpec(memory_space=pl.ANY)
    dma = pltpu.SemaphoreType.DMA

    def room(*shape, dtype=bf16):
        return pltpu.VMEM(shape, dtype)

    same = [queries, keys, values, out_weight, tokens, gate, up, down]
    return pl.pallas_call(
        fused_kernel,
        out_shape=(
            jax.ShapeDtypeStruct((share, width), bf16),
            jax.ShapeDtypeStruct((count, width), bf16),
        ),
        in_specs=[anywhere] * 3 + [vmem] * 2 + [anywhere] * 2 + [vmem] * 2 + [anywhere] * 3,
        out_specs=(vmem, vmem),
        scratch_shapes=[room(*a.shape, dtype=a.dtype) for a in same]
        + [
            room(chips, count, width),
            room(chips, *info.shape, dtype=f32),
            room(chips, peers * slots, count),
            room(chips, peers, slots, width),
            room(chips, peers, 16, count),
            room(chips, 2, peers, slots, width),
            room(chips, 2, peers, 16, count),
            room(2 * peers * slots, experts * units),
            room(chips, 2, peers, slots, width),
            room(chips, peers, slots, width),
            room(chips, peers, slots, width),
            room(chips, halves, count, half),
            room(chips + 1, halves, count, half),
            room(heads, length, DV, dtype=f32),
            room(heads, length, DK, dtype=f32),
            room(length, heads * DV),
            room(heads, DK, DV + DK),
            room(peers, heads, DK, DV + DK),
            room(heads, DK, DV, dtype=f32),
            room(2, chips, share, width),
            room(chips, share, width),
            room(chips + 1, share, width),
            dma((8,)),
            dma((5,)), dma((chips,)), dma((5,)), dma((chips,)),
            dma((chips, peers)), dma((chips, peers)), dma((chips, peers)), dma((chips, peers)),
            dma((chips,)), dma((chips,)), dma((chips,)), dma((chips,)),
            dma((chips,)), dma((chips,)),
            dma((chips, peers)), dma((chips, peers)),
            dma((chips, halves)), dma((chips + 1, halves)),
            dma((peers,)), dma((peers,)), dma, dma,
            dma((chips,)), dma((chips + 1,)),
        ],
        cost_estimate=pl.CostEstimate(
            flops=12 * chips * peers * slots * experts * units * width,
            bytes_accessed=8 * experts * units * width,
            transcendentals=0,
        ),
        compiler_params=pltpu.CompilerParams(
            collective_id=0, has_side_effects=True, vmem_limit_bytes=63 * 2**20
        ),
    )(
        queries, keys, values, strength, decay_logarithm, out_weight, tokens, scale, info,
        gate, up, down,
    )


def routing(choice, mixing, local_experts, peers):
    tokens = choice.shape[0]
    ids, parts = choice.T, mixing.T
    number = jnp.arange(peers * local_experts, dtype=jnp.int32)[:, None]
    group = jnp.arange(8, dtype=jnp.int32)[:, None]
    share = jnp.zeros((peers * local_experts, tokens), jnp.float32)
    goes = jnp.zeros((8, tokens), bool)
    for k in range(choice.shape[1]):
        share = share + jnp.where(ids[k][None] == number, parts[k][None], 0.0)
        goes = goes | (ids[k][None] // local_experts == group)
    share = share.reshape(peers, local_experts, tokens)
    share = jnp.pad(share, ((0, 0), (0, 8 - local_experts), (0, 0))).reshape(peers * 8, tokens)
    return jnp.concatenate([share, goes.astype(jnp.float32)], axis=0)


def by_tokens(normed, choice, mixing, gate, up, down, slots, after):
    ep_count = lax.axis_size("ep")
    local_experts = gate.shape[0]
    tokens, width = normed.shape
    bf16 = jnp.bfloat16
    f32 = jnp.float32
    named = choice[:, :, None] == jnp.arange(ep_count * local_experts, dtype=jnp.int32)
    share = jnp.sum(jnp.where(named, mixing[:, :, None], 0.0), axis=1)
    goes = jnp.any(named, axis=1).reshape(tokens, ep_count, local_experts).any(axis=-1)
    earlier = jnp.tril(jnp.ones((tokens, tokens), bf16), -1)
    rank = jnp.dot(earlier, goes.astype(bf16), preferred_element_type=f32)
    spread = goes[:, :, None] & (rank[:, :, None] == jnp.arange(slots, dtype=f32))
    spread = spread.astype(bf16)
    high = share.astype(bf16)
    low = (share - high.astype(f32)).astype(bf16)
    sent = jnp.einsum("tes,td->esd", spread, normed, preferred_element_type=f32).astype(bf16)
    extra = jnp.concatenate(
        [
            high.reshape(tokens, ep_count, local_experts),
            low.reshape(tokens, ep_count, local_experts),
        ],
        axis=-1,
    )
    extra = jnp.einsum("tes,tex->esx", spread, extra, preferred_element_type=f32).astype(bf16)
    pad = -extra.shape[-1] % 128
    extra = jnp.pad(extra, ((0, 0), (0, 0), (0, pad)))
    outgoing = jnp.concatenate([sent, extra], axis=-1)
    arrived = lax.all_to_all(outgoing, "ep", split_axis=0, concat_axis=0, tiled=True)
    arrived = arrived.reshape(ep_count * slots, -1)
    everyone = lax.all_gather(arrived, "tp", axis=0, tiled=True)
    produced = expert_layer(everyone, gate, up, down, arrived.shape[0])
    summed = lax.psum_scatter(produced, "tp", scatter_dimension=0, tiled=True)
    returned = lax.all_to_all(
        summed.reshape(ep_count, slots, width), "ep", split_axis=0, concat_axis=0, tiled=True
    )
    combined = jnp.einsum("tes,esd->td", spread, returned, preferred_element_type=f32)
    return combined.astype(bf16), after


def by_weights(normed, expert_choice_index, mixing, gate, up, down):
    own_tokens, width_model = normed.shape
    ep_count = lax.axis_size("ep")
    local_experts = gate.shape[0]
    experts = local_experts * ep_count
    flat_ids = expert_choice_index.reshape(-1)
    one_hot = (flat_ids[:, None] == jnp.arange(experts, dtype=jnp.int32)[None, :]).astype(jnp.int32)
    slot_rank = jnp.sum((jnp.cumsum(one_hot, axis=0) - one_hot) * one_hot, axis=1)
    slot_index = flat_ids * CAP + slot_rank
    copy_token = jnp.arange(flat_ids.shape[0], dtype=jnp.int32) // TOPK
    slot_token = jnp.full((experts * CAP,), own_tokens, jnp.int32).at[slot_index].set(copy_token)
    outgoing = jnp.take(normed, slot_token, axis=0, mode="fill", fill_value=0).reshape(
        ep_count, local_experts, CAP, width_model
    )
    arrived = lax.all_to_all(outgoing, "ep", split_axis=0, concat_axis=0, tiled=True)
    gate_piece = lax.all_gather(gate, "tp", axis=1, tiled=True)
    up_piece = lax.all_gather(up, "tp", axis=1, tiled=True)
    down_piece = lax.all_gather(down, "tp", axis=1, tiled=True)
    gating = jnp.einsum("secd,efd->secf", arrived, gate_piece, preferred_element_type=jnp.float32)
    upward = jnp.einsum("secd,efd->secf", arrived, up_piece, preferred_element_type=jnp.float32)
    hidden = (jax.nn.silu(gating) * upward).astype(jnp.bfloat16)
    produced = jnp.einsum("secf,efd->secd", hidden, down_piece, preferred_element_type=jnp.float32)
    returned = lax.all_to_all(
        produced.astype(jnp.bfloat16), "ep", split_axis=0, concat_axis=0, tiled=True
    )
    flat_results = returned.reshape(experts * CAP, width_model)
    picked = (
        jnp.take(flat_results, slot_index, axis=0)
        .reshape(own_tokens, TOPK, width_model)
        .astype(jnp.float32)
    )
    return jnp.sum(mixing[..., None] * picked, axis=1).astype(jnp.bfloat16)


def shards(
    query_heads_rows,
    key_heads_rows,
    value_heads_rows,
    write_strength_logit,
    decay_preactivation,
    head_decay_logarithm,
    extra_log_decay,
    output_weight,
    second_batch_tokens,
    expert_norm_scale,
    expert_choice_index,
    group_router_weight,
    expert_logit_difference,
    expert_gate_weight,
    expert_up_weight,
    expert_down_weight,
):
    length = query_heads_rows.shape[0]
    local_heads = head_decay_logarithm.shape[0]
    strength = jax.nn.sigmoid(write_strength_logit.astype(jnp.float32))
    decay_logarithm = (
        -jnp.exp(head_decay_logarithm)[:, None]
        * jax.nn.softplus(decay_preactivation.astype(jnp.float32))
        + extra_log_decay
    )
    leading = jax.nn.sigmoid(expert_logit_difference)
    mixing = group_router_weight[:, None] * jnp.stack([leading, 1.0 - leading], axis=-1)
    local_experts, local_units, width = expert_gate_weight.shape
    own_tokens = second_batch_tokens.shape[0]
    ep_count, tp_count = lax.axis_size("ep"), lax.axis_size("tp")
    named_both = TOPK if local_experts % EPG == 0 else 1
    slots = min(own_tokens, local_experts * CAP // named_both)
    weights = (expert_gate_weight, expert_up_weight, expert_down_weight)
    if (
        (ep_count, tp_count) == (RING, 2 * RING)
        and named_both == TOPK
        and own_tokens == DK
        and local_experts * local_units == width // RING
    ):
        return fused(
            query_heads_rows, key_heads_rows, value_heads_rows, strength, decay_logarithm,
            output_weight, second_batch_tokens, expert_norm_scale.reshape(1, width),
            routing(expert_choice_index, mixing, local_experts, ep_count), *weights, slots,
        )
    local_output, projection_matrix, end_memory = delta_rule(
        query_heads_rows, key_heads_rows, value_heads_rows, strength, decay_logarithm
    )
    incoming_rows = incoming(end_memory, "ep")
    attention_result = local_output + jnp.einsum(
        "hpg,hgd->hpd", projection_matrix, incoming_rows, precision=precise_setting
    )
    attn_rows = (
        attention_result.transpose(1, 0, 2)
        .reshape(length, local_heads * DV)
        .astype(jnp.bfloat16)
    )
    product = jnp.dot(attn_rows, output_weight, preferred_element_type=jnp.float32)
    product = product.astype(jnp.bfloat16)
    widened = second_batch_tokens.astype(jnp.float32)
    normed = (
        widened
        * lax.rsqrt(jnp.mean(widened * widened, axis=-1, keepdims=True) + norm_eps)
        * expert_norm_scale
    ).astype(jnp.bfloat16)
    if 2 * tp_count * ep_count * slots < 3 * local_experts * local_units * tp_count:
        expert_out, product = by_tokens(
            normed, expert_choice_index, mixing, *weights, slots, product
        )
    else:
        expert_out = by_weights(normed, expert_choice_index, mixing, *weights)
    summed = lax.psum_scatter(product, "tp", scatter_dimension=0, tiled=True)
    return (summed, expert_out)


def solution(mesh):
    in_specs = (
        P("ep", "tp"),
        P("ep", "tp"),
        P("ep", "tp"),
        P("tp", "ep"),
        P("tp", "ep"),
        P("tp"),
        P("tp", "ep"),
        P("tp", None),
        P(("ep", "tp"), None),
        P(),
        P(("ep", "tp"), None),
        P(("ep", "tp")),
        P(("ep", "tp")),
        P("ep", "tp", None),
        P("ep", "tp", None),
        P("ep", "tp", None),
    )
    out_specs = (P(("ep", "tp"), None), P(("ep", "tp"), None))
    return jax.shard_map(shards, mesh=mesh, in_specs=in_specs, out_specs=out_specs, check_vma=False)
```

```python
import functools

import jax
import jax.numpy as jnp
from jax import lax
from jax.experimental import pallas as pl
from jax.experimental.pallas import tpu as pltpu
from jax.sharding import PartitionSpec as P

DK = 128
DV = 128
CAP = 32
RING = 4
MESH = pl.DeviceIdType.MESH
EPG = 4
TOPK = 2


precise_setting = lax.Precision.HIGHEST
norm_eps = 1e-06


def incoming(end_memory, axis):
    count, mine = (lax.axis_size(axis), lax.axis_index(axis))
    pieces = lax.all_gather(end_memory, axis)
    state = jnp.zeros(end_memory.shape[:-1] + (DV,), jnp.float32)
    for position in range(count - 1):
        end, transfer = pieces[position, ..., :DV], pieces[position, ..., DV:]
        longer = end + jnp.einsum("hij,hjv->hiv", transfer, state, precision=precise_setting)
        state = jnp.where(position < mine, longer, state)
    return state


def unit_rows(matrix):
    return matrix * lax.rsqrt(jnp.sum(matrix * matrix, axis=-1, keepdims=True) + norm_eps)


def mm(a, b, dims=((1,), (0,))):
    return lax.dot_general(
        a, b, (dims, ((), ())), precision=precise_setting, preferred_element_type=jnp.float32
    )


def delta_body(q_ref, k_ref, v_ref, strength_ref, decay_ref, local_ref, proj_ref, end_ref):
    heads = strength_ref.shape[0]
    chunk = DK
    chunks = q_ref.shape[0] // chunk
    rows = lax.broadcasted_iota(jnp.int32, (chunk, chunk), 0)
    cols = lax.broadcasted_iota(jnp.int32, (chunk, chunk), 1)
    within = rows >= cols
    eye = jnp.where(rows == cols, 1.0, 0.0)
    parts = []
    for h in range(heads):
        for c in range(chunks):
            at = pl.ds(c * chunk, chunk)
            q = q_ref[at, h * DK : (h + 1) * DK].astype(jnp.float32)
            k = k_ref[at, h * DK : (h + 1) * DK].astype(jnp.float32)
            v = v_ref[at, h * DV : (h + 1) * DV].astype(jnp.float32)
            q = unit_rows(q) * DK ** (-0.5)
            k = unit_rows(k)
            d_row = decay_ref[h : h + 1, c * chunk : (c + 1) * chunk]
            b_row = strength_ref[h : h + 1, c * chunk : (c + 1) * chunk]
            d_col = jnp.sum(jnp.where(rows == cols, d_row, 0.0), axis=1, keepdims=True)
            b_col = jnp.sum(jnp.where(rows == cols, b_row, 0.0), axis=1, keepdims=True)
            cum_col = jnp.sum(jnp.where(within, d_row, 0.0), axis=1, keepdims=True)
            cum_row = jnp.sum(jnp.where(rows <= cols, d_col, 0.0), axis=0, keepdims=True)
            last = cum_col[chunk - 1 : chunk, :]
            decayed = jnp.where(within, jnp.exp(jnp.where(within, cum_col - cum_row, 0.0)), 0.0)
            weighted = k * b_col
            lower = jnp.where(
                rows > cols, mm(weighted, k, ((1,), (1,))) * decayed, 0.0
            )
            scores = mm(q, k, ((1,), (1,))) * decayed
            grown = jnp.exp(cum_col)
            rhs = jnp.concatenate([v * b_col, weighted * grown], axis=1)
            parts.append([lower, scores, rhs, q * grown, k * jnp.exp(last - cum_col), jnp.exp(last)])
    inverses = [None] * len(parts)
    span = 1
    while span < chunk:
        mask = (
            (rows // (2 * span) == cols // (2 * span))
            & (rows // span % 2 == 1)
            & (cols // span % 2 == 0)
        )
        for i, part in enumerate(parts):
            edge = jnp.where(mask, part[0], 0.0)
            if span == 1:
                inverses[i] = eye - edge
            else:
                inverses[i] = inverses[i] - mm(mm(inverses[i], edge), inverses[i])
        span *= 2
    solved = [mm(inverse, part[2]) for inverse, part in zip(inverses, parts)]
    yield
    states = [
        jnp.concatenate([jnp.zeros((DK, DV), jnp.float32), eye], axis=1) for _ in range(heads)
    ]
    for c in range(chunks):
        for h in range(heads):
            _, scores, _, queries, keys, retention = parts[h * chunks + c]
            both = solved[h * chunks + c]
            fresh = jnp.concatenate([both[:, :DV], jnp.zeros((chunk, DK), jnp.float32)], axis=1)
            state = states[h]
            updates = fresh - mm(both[:, DV:], state)
            out = mm(queries, state) + mm(scores, updates)
            states[h] = state * retention + mm(keys, updates, ((0,), (0,)))
            at = pl.ds(c * chunk, chunk)
            local_ref[h, at, :] = out[:, :DV]
            proj_ref[h, at, :] = out[:, DV:]
    for h in range(heads):
        end_ref[h] = states[h].astype(end_ref.dtype)
    yield


def delta_kernel(*refs):
    for _ in delta_body(*refs):
        pass


def delta_rule(queries, keys, values, strength, decay_logarithm):
    heads, length = strength.shape
    vmem = pl.BlockSpec(memory_space=pltpu.VMEM)
    f32 = jnp.float32
    return pl.pallas_call(
        delta_kernel,
        out_shape=(
            jax.ShapeDtypeStruct((heads, length, DV), f32),
            jax.ShapeDtypeStruct((heads, length, DK), f32),
            jax.ShapeDtypeStruct((heads, DK, DV + DK), f32),
        ),
        in_specs=[vmem] * 5,
        out_specs=(vmem,) * 3,
        cost_estimate=pl.CostEstimate(
            flops=40 * heads * length * DK * DK * 6, bytes_accessed=4 * 2**20, transcendentals=0
        ),
        compiler_params=pltpu.CompilerParams(vmem_limit_bytes=40 * 2**20),
    )(queries, keys, values, strength, decay_logarithm)


def expert_kernel(x_ref, gate_ref, up_ref, down_ref, out_ref):
    experts, units, width = gate_ref.shape
    x = x_ref[:, :width]
    hidden = []
    for e in range(experts):
        gating = lax.dot_general(
            x, gate_ref[e], (((1,), (1,)), ((), ())), preferred_element_type=jnp.float32
        )
        upward = lax.dot_general(
            x, up_ref[e], (((1,), (1,)), ((), ())), preferred_element_type=jnp.float32
        )
        share = x_ref[:, width + e : width + e + 1].astype(jnp.float32) + x_ref[
            :, width + experts + e : width + experts + e + 1
        ].astype(jnp.float32)
        hidden.append((gating / (1.0 + jnp.exp(-gating)) * upward * share).astype(jnp.bfloat16))
    hidden = jnp.concatenate(hidden, axis=1)
    down = down_ref[...].reshape(experts * units, width)
    out_ref[...] = jnp.dot(hidden, down, preferred_element_type=jnp.float32).astype(jnp.bfloat16)


def expert_layer(rows, gate, up, down, tile):
    count, wide = rows.shape
    experts, units, width = gate.shape
    whole = pl.BlockSpec((experts, units, width), lambda i: (0, 0, 0))
    return pl.pallas_call(
        expert_kernel,
        grid=(count // tile,),
        out_shape=jax.ShapeDtypeStruct((count, width), jnp.bfloat16),
        in_specs=[pl.BlockSpec((tile, wide), lambda i: (i, 0)), whole, whole, whole],
        out_specs=pl.BlockSpec((tile, width), lambda i: (i, 0)),
        cost_estimate=pl.CostEstimate(
            flops=6 * count * experts * units * width,
            bytes_accessed=4 * count * width + 6 * experts * units * width,
            transcendentals=0,
        ),
        compiler_params=pltpu.CompilerParams(vmem_limit_bytes=48 * 2**20),
    )(rows, gate, up, down)


def routing(choice, router, difference, experts, peers):
    tokens = choice.shape[1]
    f32, i32 = jnp.float32, jnp.int32
    ids = choice.astype(f32)
    leading = 1.0 / (1.0 + jnp.exp(-difference))
    parts = (router * leading, router * (1.0 - leading))
    line = lax.broadcasted_iota(i32, (peers * 8, tokens), 0)
    within = lax.rem(line, 8)
    number = jnp.where(within < experts, line // 8 * experts + within, -1).astype(f32)
    first = (lax.broadcasted_iota(i32, (8, tokens), 0) * experts).astype(f32)
    share = jnp.zeros((peers * 8, tokens), f32)
    goes = jnp.zeros((8, tokens), f32)
    for k in range(TOPK):
        named = ids[k : k + 1]
        share = share + jnp.where(named == number, parts[k], 0.0)
        inside = jnp.logical_and(named >= first, named < first + experts)
        goes = jnp.where(inside, 1.0, goes)
    return jnp.concatenate([share, goes], axis=0)


def fused_kernel(*refs):
    arguments, (mixed_ref, expert_ref), rest = refs[:16], refs[16:18], refs[18:]
    copies, rest = rest[:16], rest[16:]
    (
        tokens_ref, scale_ref, choice_ref, router_ref, difference_ref, logit_ref, before_ref,
        rate_ref, extra_ref, q_ref, k_ref, v_ref, gate_ref, up_ref, down_ref, wout_ref,
    ) = copies
    (
        raw, infos, spreads, stage, stage_share, rows, rows_share, hid, res, theirs, back,
        acc, inb, local, proj, attn, states_out, states_in, state, prod, prod_theirs, mixed_in,
        strength_ref, decay_ref, load_sems, ag_s, ag_r, agi_s, agi_r, ep_s, ep_r, eps_s, eps_r, core_s, core_r, cores_s, cores_r,
        pair_s, pair_r, back_s, back_r, rs_s, rs_r, st_s, st_r, pp_s, pp_r, mr_s, mr_r,
    ) = rest
    e, t = lax.axis_index("ep"), lax.axis_index("tp")
    core, z = lax.rem(t, 2), lax.div(t, 2)
    chips, tokens, width = raw.shape
    peers, slots = stage.shape[1], stage.shape[2]
    experts, units, _ = gate_ref.shape
    count = peers * slots
    pieces, part = acc.shape[1], acc.shape[3]
    last = chips - 1
    bf16, f32 = jnp.bfloat16, jnp.float32
    upper = lax.div(z, 2)
    near_end = z + upper * (last - 2 * z)

    def order(i):
        base = (near_end, 1 + 2 * near_end, 3 - 3 * near_end, 2)[i]
        return base + upper * (last - 2 * base)

    swap = (1 - near_end) * (order(2) - order(1))
    returns = (order(1) + swap, order(3), order(2) - swap)
    inner = jnp.logical_and(z >= 1, z <= last - 1)
    outer = jnp.logical_or(z == 0, z == last)
    other = (e, z * 2 + 1 - core)

    def at_chip(chip):
        return (e, chip * 2 + core)

    def at_peer(j):
        return (lax.rem(e + j, peers), t)

    sources = [lax.rem(e + peers - j, peers) for j in range(peers)]

    loads = []
    for i, (src, dst) in enumerate(zip(arguments, copies)):
        copy = pltpu.make_async_copy(src, dst, load_sems.at[i])
        copy.start()
        loads.append(copy)

    barrier = pltpu.get_barrier_semaphore()
    greeted = [at_peer(j) for j in range(1, peers)] + [other]
    greeted += [at_chip(lax.rem(z + h, chips)) for h in range(1, chips)]
    for device in greeted:
        pl.semaphore_signal(barrier, inc=1, device_id=device, device_id_type=MESH)

    started = []

    def send(src, dst, send_sem, recv_sem, device, when=None):
        def make():
            return pltpu.make_async_remote_copy(
                src_ref=src, dst_ref=dst, send_sem=send_sem, recv_sem=recv_sem,
                device_id=device, device_id_type=MESH,
            )

        if when is None:
            make().start()
        else:
            @pl.when(when)
            def _():
                make().start()
        started.append((make, when))

    def arrived(dst, send_sem, recv_sem):
        pltpu.make_async_remote_copy(
            src_ref=dst, dst_ref=dst, send_sem=send_sem, recv_sem=recv_sem,
            device_id=other, device_id_type=MESH,
        ).wait_recv()

    for copy in loads[:5]:
        copy.wait()
    widened = tokens_ref[...].astype(f32)
    raw[z] = (
        widened
        * lax.rsqrt(jnp.mean(widened * widened, axis=-1, keepdims=True) + norm_eps)
        * scale_ref[...]
    ).astype(bf16)
    infos[z] = routing(
        choice_ref[...], router_ref[...], difference_ref[...], experts, peers
    )
    pl.semaphore_wait(barrier, len(greeted))

    step = 1 - 2 * upper

    def share_rows(n, chip, target, when):
        device = at_chip(target)
        send(infos.at[chip], infos.at[chip], agi_s.at[n], agi_r.at[chip], device, when)
        send(raw.at[chip], raw.at[chip], ag_s.at[n], ag_r.at[chip], device, when)

    share_rows(0, z, z + 2 * step, outer)
    share_rows(1, z, z + step, outer)
    share_rows(2, z, z - step, inner)

    def gathered(chip):
        arrived(infos.at[chip], agi_s.at[0], agi_r.at[chip])
        arrived(raw.at[chip], ag_s.at[0], ag_r.at[chip])

    def select(chip):
        info = infos[chip]
        goes = info[peers * 8 : peers * 8 + 8]
        before = lax.broadcasted_iota(jnp.int32, (tokens, tokens), 0) < lax.broadcasted_iota(
            jnp.int32, (tokens, tokens), 1
        )
        rank = jnp.dot(
            goes.astype(bf16), jnp.where(before, 1.0, 0.0).astype(bf16), preferred_element_type=f32
        )
        slot = lax.broadcasted_iota(jnp.int32, (tokens, tokens), 0).astype(f32)
        for g in range(peers):
            hit = jnp.logical_and(slot == rank[g : g + 1], goes[g : g + 1] > 0.5)
            spread = jnp.where(hit, 1.0, 0.0)
            share = mm(info[g * 8 : g * 8 + 8], spread, ((1,), (1,)))
            high = share.astype(bf16)
            low = (share - high.astype(f32)).astype(bf16)
            stage_share[chip, g] = jnp.concatenate([high, low], axis=0)
            spreads[chip, g * slots : (g + 1) * slots] = spread[:slots].astype(bf16)

        def columns(n, carry):
            at = pl.ds(pl.multiple_of(n * 512, 512), 512)
            picked = jnp.dot(spreads[chip], raw[chip, :, at], preferred_element_type=f32)
            stage[chip, :, :, at] = picked.astype(bf16).reshape(peers, slots, 512)
            return carry

        lax.fori_loop(0, width // 512, columns, 0)
        for j in (3, 1, 2):
            target = lax.rem(e + j, peers)
            send(
                stage_share.at[chip, target], rows_share.at[chip, core, e],
                eps_s.at[chip, j], eps_r.at[chip, j], (target, t),
            )
            send(
                stage.at[chip, target], rows.at[chip, core, e],
                ep_s.at[chip, j], ep_r.at[chip, j], (target, t),
            )
        rows[chip, core, e] = stage[chip, e]
        rows_share[chip, core, e] = stage_share[chip, e]

    def pass_on(chip):
        for j in range(1, peers):
            arrived(rows_share.at[chip, core, sources[j]], eps_s.at[chip, j], eps_r.at[chip, j])
            arrived(rows.at[chip, core, sources[j]], ep_s.at[chip, j], ep_r.at[chip, j])
        send(
            rows_share.at[chip, core], rows_share.at[chip, core],
            cores_s.at[chip], cores_r.at[chip], other,
        )
        send(rows.at[chip, core], rows.at[chip, core], core_s.at[chip], core_r.at[chip], other)

    def produce(chip):
        arrived(rows_share.at[chip, 1 - core], cores_s.at[chip], cores_r.at[chip])
        arrived(rows.at[chip, 1 - core], core_s.at[chip], core_r.at[chip])
        unit = lax.broadcasted_iota(jnp.int32, (16, 2 * units), 1) // units
        which = lax.rem(lax.broadcasted_iota(jnp.int32, (16, 2 * units), 0), 8)

        def expert_pair(n, carry):
            pick = jnp.where(which == unit + 2 * n, 1.0, 0.0).astype(bf16)
            share = [
                lax.dot_general(
                    rows_share[chip, c, p], pick, (((0,), (0,)), ((), ())),
                    preferred_element_type=f32,
                )[:slots]
                for c in range(2)
                for p in range(peers)
            ]
            share = jnp.concatenate(share, axis=0)
            x = rows[chip].reshape(2 * count, width)
            gating = lax.dot_general(
                x, gate_ref[pl.ds(2 * n, 2)].reshape(2 * units, width),
                (((1,), (1,)), ((), ())), preferred_element_type=f32,
            )
            upward = lax.dot_general(
                x, up_ref[pl.ds(2 * n, 2)].reshape(2 * units, width),
                (((1,), (1,)), ((), ())), preferred_element_type=f32,
            )
            at = pl.ds(pl.multiple_of(n * 2 * units, 2 * units), 2 * units)
            hid[:, at] = (gating / (1.0 + jnp.exp(-gating)) * upward * share).astype(bf16)
            return carry

        lax.fori_loop(0, experts // 2, expert_pair, 0)

        def columns(n, carry):
            at = pl.ds(pl.multiple_of(n * 512, 512), 512)
            down = down_ref[:, :, at].reshape(experts * units, 512)
            made = jnp.dot(hid[...], down, preferred_element_type=f32)
            res[chip, :, :, :, at] = made.astype(bf16).reshape(2, peers, slots, 512)
            return carry

        lax.fori_loop(0, width // 512, columns, 0)
        send(res.at[chip, 1 - core], theirs.at[chip], pair_s.at[chip], pair_r.at[chip], other)

    def give_back(chip):
        arrived(theirs.at[chip], pair_s.at[chip], pair_r.at[chip])
        res[chip, core] = (res[chip, core].astype(f32) + theirs[chip].astype(f32)).astype(bf16)
        for j in (3, 1, 2):
            target = lax.rem(e + j, peers)
            send(
                res.at[chip, core, target], back.at[chip, e],
                back_s.at[chip, j], back_r.at[chip, j], (target, t),
            )
        back[chip, e] = res[chip, core, e]

    def unselect(chip):
        for j in range(1, peers):
            arrived(back.at[chip, sources[j]], back_s.at[chip, j], back_r.at[chip, j])
        for h in range(pieces):
            acc[chip, h] = lax.dot_general(
                spreads[chip],
                back[chip, :, :, h * part : (h + 1) * part].reshape(count, part),
                (((0,), (0,)), ((), ())), preferred_element_type=f32,
            ).astype(bf16)

    def add_from(total, piece, send_sem, recv_sem):
        @pl.when(inner)
        def _():
            arrived(piece, send_sem, recv_sem)
            total[...] = (total[...].astype(f32) + piece[...].astype(f32)).astype(bf16)

    def forward(chip, joins):
        device = at_chip(chip)
        if joins:
            device = at_chip(z + step + near_end * (chip - z - step))
        slot = chip + (near_end * (chips - chip) if joins else 0)
        for h in range(pieces):
            if joins:
                add_from(acc.at[chip, h], inb.at[chip, h], rs_s.at[chip, h], rs_r.at[chip, h])
            send(acc.at[chip, h], inb.at[slot, h], rs_s.at[chip, h], rs_r.at[slot, h], device)

    def finish(first, parts, sems, out, at):
        total = first[...].astype(f32)
        for piece, sem in zip(parts, sems[1:]):
            arrived(piece, sems[0], sem)
            total = total + piece[...].astype(f32)
        out[:, at] = total.astype(bf16)

    heads = local.shape[0]

    def send_states():
        for j in range(1, peers):
            send(states_out, states_in.at[j], st_s.at[j], st_r.at[j], at_peer(j), e < peers - j)

    def project():
        state[...] = jnp.zeros_like(state)
        for j in range(peers - 1, 0, -1):
            @pl.when(e >= j)
            def _():
                arrived(states_in.at[j], st_s.at[j], st_r.at[j])
                for h in range(heads):
                    piece = states_in[j, h].astype(f32)
                    state[h] = piece[:, :DV] + mm(piece[:, DV:], state[h])
        for h in range(heads):
            attn[:, h * DV : (h + 1) * DV] = (local[h] + mm(proj[h], state[h])).astype(bf16)
        loads[15].wait()
        share = prod.shape[2]

        def columns(n, carry):
            at = pl.ds(pl.multiple_of(n * 512, 512), 512)
            made = jnp.dot(attn[...], wout_ref[:, at], preferred_element_type=f32)
            made = made.astype(bf16).reshape(chips, 2, share, 512)
            for c in range(2):
                prod[c, :, :, at] = made[:, c]
            return carry

        lax.fori_loop(0, width // 512, columns, 0)
        send(prod.at[1 - core], prod_theirs, pp_s, pp_r, other)

    def join_mixed():
        arrived(prod_theirs, pp_s, pp_r)
        prod[core] = (prod[core].astype(f32) + prod_theirs[...].astype(f32)).astype(bf16)

    def send_mixed(chip, slot, target, when):
        send(
            prod.at[core, chip], mixed_in.at[slot],
            mr_s.at[chip], mr_r.at[slot], at_chip(target), when,
        )

    def start_mixed():
        for n in (3, 2, 1):
            send_mixed(z + n * step, z + n * step, z + step, outer)
        send_mixed(z - step, z - step, z - step, inner)

    def pass_mixed():
        for n in (2, 1):
            chip = z + n * step

            @pl.when(inner)
            def _():
                arrived(mixed_in.at[chip], mr_s.at[chip], mr_r.at[chip])
                prod[core, chip] = (
                    prod[core, chip].astype(f32) + mixed_in[chip].astype(f32)
                ).astype(bf16)

            send_mixed(chip, chips, chip, inner)

    select(order(0))
    for copy in loads[5:12]:
        copy.wait()
    strength_ref[...] = 1.0 / (1.0 + jnp.exp(-logit_ref[...].astype(f32)))
    before = before_ref[...].astype(f32)
    growth = jnp.maximum(before, 0.0) + jnp.log1p(jnp.exp(-jnp.abs(before)))
    for h in range(heads):
        decay_ref[h : h + 1] = (
            -jnp.exp(rate_ref[:, h : h + 1]) * growth[h : h + 1] + extra_ref[h : h + 1]
        )
    delta = delta_body(q_ref, k_ref, v_ref, strength_ref, decay_ref, local, proj, states_out)
    next(delta)
    gathered(order(1))
    share_rows(3, order(1), z - step, inner)
    share_rows(1, z, z + step, inner)
    select(order(1))
    next(delta)
    send_states()
    pass_on(order(0))
    for copy in loads[12:15]:
        copy.wait()
    produce(order(0))
    gathered(order(2))
    share_rows(0, z, z + 2 * step, inner)
    select(order(2))
    pass_on(order(1))
    produce(order(1))
    gathered(order(3))
    select(order(3))
    project()
    pass_on(order(2))
    produce(order(2))
    join_mixed()
    start_mixed()
    give_back(returns[0])
    pass_on(order(3))
    produce(order(3))
    give_back(returns[1])
    give_back(returns[2])
    give_back(order(0))
    pass_mixed()
    unselect(returns[0])
    forward(returns[0], True)
    unselect(returns[1])
    forward(returns[1], True)
    finish(
        prod.at[core, z], (mixed_in.at[z], mixed_in.at[chips]),
        (mr_s.at[0], mr_r.at[z], mr_r.at[chips]), mixed_ref, slice(0, width),
    )
    unselect(returns[2])
    forward(returns[2], False)
    unselect(order(0))
    for h in range(pieces):
        finish(
            acc.at[z, h], (inb.at[z, h], inb.at[chips, h]),
            (rs_s.at[0, h], rs_r.at[z, h], rs_r.at[chips, h]),
            expert_ref, slice(h * part, (h + 1) * part),
        )
    for make, when in started:
        if when is None:
            make().wait_send()
        else:
            @pl.when(when)
            def _():
                make().wait_send()


def fused(
    tokens, scale, choice, router, difference, logit, before, rate, extra,
    queries, keys, values, gate, up, down, out_weight, slots,
):
    experts, units, width = gate.shape
    count, peers, chips, pieces = tokens.shape[0], lax.axis_size("ep"), RING, 4
    heads, length = extra.shape
    part = width // pieces
    share = length // (2 * chips)
    bf16, f32 = jnp.bfloat16, jnp.float32
    vmem = pl.BlockSpec(memory_space=pltpu.VMEM)
    anywhere = pl.BlockSpec(memory_space=pl.ANY)
    dma = pltpu.SemaphoreType.DMA

    def room(*shape, dtype=bf16):
        return pltpu.VMEM(shape, dtype)

    arguments = [
        tokens, scale, choice, router, difference, logit, before, rate, extra,
        queries, keys, values, gate, up, down, out_weight,
    ]
    return pl.pallas_call(
        fused_kernel,
        out_shape=(
            jax.ShapeDtypeStruct((share, width), bf16),
            jax.ShapeDtypeStruct((count, width), bf16),
        ),
        in_specs=[anywhere] * len(arguments),
        out_specs=(vmem, vmem),
        scratch_shapes=[room(*a.shape, dtype=a.dtype) for a in arguments]
        + [
            room(chips, count, width),
            room(chips, (peers + 1) * 8, count, dtype=f32),
            room(chips, peers * slots, count),
            room(chips, peers, slots, width),
            room(chips, peers, 16, count),
            room(chips, 2, peers, slots, width),
            room(chips, 2, peers, 16, count),
            room(2 * peers * slots, experts * units),
            room(chips, 2, peers, slots, width),
            room(chips, peers, slots, width),
            room(chips, peers, slots, width),
            room(chips, pieces, count, part),
            room(chips + 1, pieces, count, part),
            room(heads, length, DV, dtype=f32),
            room(heads, length, DK, dtype=f32),
            room(length, heads * DV),
            room(heads, DK, DV + DK),
            room(peers, heads, DK, DV + DK),
            room(heads, DK, DV, dtype=f32),
            room(2, chips, share, width),
            room(chips, share, width),
            room(chips + 1, share, width),
            room(heads, length, dtype=f32),
            room(heads, length, dtype=f32),
            dma((len(arguments),)),
            dma((5,)), dma((chips,)), dma((5,)), dma((chips,)),
            dma((chips, peers)), dma((chips, peers)), dma((chips, peers)), dma((chips, peers)),
            dma((chips,)), dma((chips,)), dma((chips,)), dma((chips,)),
            dma((chips,)), dma((chips,)),
            dma((chips, peers)), dma((chips, peers)),
            dma((chips, pieces)), dma((chips + 1, pieces)),
            dma((peers,)), dma((peers,)), dma, dma,
            dma((chips,)), dma((chips + 1,)),
        ],
        cost_estimate=pl.CostEstimate(
            flops=12 * chips * peers * slots * experts * units * width,
            bytes_accessed=8 * experts * units * width,
            transcendentals=0,
        ),
        compiler_params=pltpu.CompilerParams(
            collective_id=0, has_side_effects=True, vmem_limit_bytes=63 * 2**20
        ),
    )(*arguments)


def by_tokens(normed, choice, mixing, gate, up, down, slots, after):
    ep_count = lax.axis_size("ep")
    local_experts = gate.shape[0]
    tokens, width = normed.shape
    bf16 = jnp.bfloat16
    f32 = jnp.float32
    named = choice[:, :, None] == jnp.arange(ep_count * local_experts, dtype=jnp.int32)
    share = jnp.sum(jnp.where(named, mixing[:, :, None], 0.0), axis=1)
    goes = jnp.any(named, axis=1).reshape(tokens, ep_count, local_experts).any(axis=-1)
    earlier = jnp.tril(jnp.ones((tokens, tokens), bf16), -1)
    rank = jnp.dot(earlier, goes.astype(bf16), preferred_element_type=f32)
    spread = goes[:, :, None] & (rank[:, :, None] == jnp.arange(slots, dtype=f32))
    spread = spread.astype(bf16)
    high = share.astype(bf16)
    low = (share - high.astype(f32)).astype(bf16)
    sent = jnp.einsum("tes,td->esd", spread, normed, preferred_element_type=f32).astype(bf16)
    extra = jnp.concatenate(
        [
            high.reshape(tokens, ep_count, local_experts),
            low.reshape(tokens, ep_count, local_experts),
        ],
        axis=-1,
    )
    extra = jnp.einsum("tes,tex->esx", spread, extra, preferred_element_type=f32).astype(bf16)
    pad = -extra.shape[-1] % 128
    extra = jnp.pad(extra, ((0, 0), (0, 0), (0, pad)))
    outgoing = jnp.concatenate([sent, extra], axis=-1)
    arrived = lax.all_to_all(outgoing, "ep", split_axis=0, concat_axis=0, tiled=True)
    arrived = arrived.reshape(ep_count * slots, -1)
    everyone = lax.all_gather(arrived, "tp", axis=0, tiled=True)
    produced = expert_layer(everyone, gate, up, down, arrived.shape[0])
    summed = lax.psum_scatter(produced, "tp", scatter_dimension=0, tiled=True)
    returned = lax.all_to_all(
        summed.reshape(ep_count, slots, width), "ep", split_axis=0, concat_axis=0, tiled=True
    )
    combined = jnp.einsum("tes,esd->td", spread, returned, preferred_element_type=f32)
    return combined.astype(bf16), after


def by_weights(normed, expert_choice_index, mixing, gate, up, down):
    own_tokens, width_model = normed.shape
    ep_count = lax.axis_size("ep")
    local_experts = gate.shape[0]
    experts = local_experts * ep_count
    flat_ids = expert_choice_index.reshape(-1)
    one_hot = (flat_ids[:, None] == jnp.arange(experts, dtype=jnp.int32)[None, :]).astype(jnp.int32)
    slot_rank = jnp.sum((jnp.cumsum(one_hot, axis=0) - one_hot) * one_hot, axis=1)
    slot_index = flat_ids * CAP + slot_rank
    copy_token = jnp.arange(flat_ids.shape[0], dtype=jnp.int32) // TOPK
    slot_token = jnp.full((experts * CAP,), own_tokens, jnp.int32).at[slot_index].set(copy_token)
    outgoing = jnp.take(normed, slot_token, axis=0, mode="fill", fill_value=0).reshape(
        ep_count, local_experts, CAP, width_model
    )
    arrived = lax.all_to_all(outgoing, "ep", split_axis=0, concat_axis=0, tiled=True)
    gate_piece = lax.all_gather(gate, "tp", axis=1, tiled=True)
    up_piece = lax.all_gather(up, "tp", axis=1, tiled=True)
    down_piece = lax.all_gather(down, "tp", axis=1, tiled=True)
    gating = jnp.einsum("secd,efd->secf", arrived, gate_piece, preferred_element_type=jnp.float32)
    upward = jnp.einsum("secd,efd->secf", arrived, up_piece, preferred_element_type=jnp.float32)
    hidden = (jax.nn.silu(gating) * upward).astype(jnp.bfloat16)
    produced = jnp.einsum("secf,efd->secd", hidden, down_piece, preferred_element_type=jnp.float32)
    returned = lax.all_to_all(
        produced.astype(jnp.bfloat16), "ep", split_axis=0, concat_axis=0, tiled=True
    )
    flat_results = returned.reshape(experts * CAP, width_model)
    picked = (
        jnp.take(flat_results, slot_index, axis=0)
        .reshape(own_tokens, TOPK, width_model)
        .astype(jnp.float32)
    )
    return jnp.sum(mixing[..., None] * picked, axis=1).astype(jnp.bfloat16)


def shards(
    query_heads_rows,
    key_heads_rows,
    value_heads_rows,
    write_strength_logit,
    decay_preactivation,
    head_decay_logarithm,
    extra_log_decay,
    output_weight,
    second_batch_tokens,
    expert_norm_scale,
    expert_choice_index,
    group_router_weight,
    expert_logit_difference,
    expert_gate_weight,
    expert_up_weight,
    expert_down_weight,
):
    length = query_heads_rows.shape[0]
    local_heads = head_decay_logarithm.shape[0]
    strength = jax.nn.sigmoid(write_strength_logit.astype(jnp.float32))
    decay_logarithm = (
        -jnp.exp(head_decay_logarithm)[:, None]
        * jax.nn.softplus(decay_preactivation.astype(jnp.float32))
        + extra_log_decay
    )
    leading = jax.nn.sigmoid(expert_logit_difference)
    mixing = group_router_weight[:, None] * jnp.stack([leading, 1.0 - leading], axis=-1)
    local_experts, local_units, width = expert_gate_weight.shape
    own_tokens = second_batch_tokens.shape[0]
    ep_count, tp_count = lax.axis_size("ep"), lax.axis_size("tp")
    named_both = TOPK if local_experts % EPG == 0 else 1
    slots = min(own_tokens, local_experts * CAP // named_both)
    weights = (expert_gate_weight, expert_up_weight, expert_down_weight)
    if (
        (ep_count, tp_count) == (RING, 2 * RING)
        and named_both == TOPK
        and own_tokens == DK
        and local_experts * local_units == width // RING
    ):
        return fused(
            second_batch_tokens, expert_norm_scale.reshape(1, width), expert_choice_index.T,
            group_router_weight.reshape(1, own_tokens),
            expert_logit_difference.reshape(1, own_tokens),
            write_strength_logit, decay_preactivation,
            head_decay_logarithm.reshape(1, local_heads), extra_log_decay,
            query_heads_rows, key_heads_rows, value_heads_rows, *weights, output_weight, slots,
        )
    local_output, projection_matrix, end_memory = delta_rule(
        query_heads_rows, key_heads_rows, value_heads_rows, strength, decay_logarithm
    )
    incoming_rows = incoming(end_memory, "ep")
    attention_result = local_output + jnp.einsum(
        "hpg,hgd->hpd", projection_matrix, incoming_rows, precision=precise_setting
    )
    attn_rows = (
        attention_result.transpose(1, 0, 2)
        .reshape(length, local_heads * DV)
        .astype(jnp.bfloat16)
    )
    product = jnp.dot(attn_rows, output_weight, preferred_element_type=jnp.float32)
    product = product.astype(jnp.bfloat16)
    widened = second_batch_tokens.astype(jnp.float32)
    normed = (
        widened
        * lax.rsqrt(jnp.mean(widened * widened, axis=-1, keepdims=True) + norm_eps)
        * expert_norm_scale
    ).astype(jnp.bfloat16)
    if 2 * tp_count * ep_count * slots < 3 * local_experts * local_units * tp_count:
        expert_out, product = by_tokens(
            normed, expert_choice_index, mixing, *weights, slots, product
        )
    else:
        expert_out = by_weights(normed, expert_choice_index, mixing, *weights)
    summed = lax.psum_scatter(product, "tp", scatter_dimension=0, tiled=True)
    return (summed, expert_out)


def solution(mesh):
    in_specs = (
        P("ep", "tp"),
        P("ep", "tp"),
        P("ep", "tp"),
        P("tp", "ep"),
        P("tp", "ep"),
        P("tp"),
        P("tp", "ep"),
        P("tp", None),
        P(("ep", "tp"), None),
        P(),
        P(("ep", "tp"), None),
        P(("ep", "tp")),
        P(("ep", "tp")),
        P("ep", "tp", None),
        P("ep", "tp", None),
        P("ep", "tp", None),
    )
    out_specs = (P(("ep", "tp"), None), P(("ep", "tp"), None))
    return jax.shard_map(shards, mesh=mesh, in_specs=in_specs, out_specs=out_specs, check_vma=False)
```

```python
import functools

import jax
import jax.numpy as jnp
from jax import lax
from jax.experimental import pallas as pl
from jax.experimental.pallas import tpu as pltpu
from jax.sharding import PartitionSpec as P

DK = 128
DV = 128
CAP = 32
RING = 4
MESH = pl.DeviceIdType.MESH
EPG = 4
TOPK = 2


precise_setting = lax.Precision.HIGHEST
norm_eps = 1e-06


def incoming(end_memory, axis):
    count, mine = (lax.axis_size(axis), lax.axis_index(axis))
    pieces = lax.all_gather(end_memory, axis)
    state = jnp.zeros(end_memory.shape[:-1] + (DV,), jnp.float32)
    for position in range(count - 1):
        end, transfer = pieces[position, ..., :DV], pieces[position, ..., DV:]
        longer = end + jnp.einsum("hij,hjv->hiv", transfer, state, precision=precise_setting)
        state = jnp.where(position < mine, longer, state)
    return state


def unit_rows(matrix):
    return matrix * lax.rsqrt(jnp.sum(matrix * matrix, axis=-1, keepdims=True) + norm_eps)


def mm(a, b, dims=((1,), (0,))):
    return lax.dot_general(
        a, b, (dims, ((), ())), precision=precise_setting, preferred_element_type=jnp.float32
    )


def delta_body(q_ref, k_ref, v_ref, strength_ref, decay_ref, local_ref, proj_ref, end_ref):
    heads = strength_ref.shape[0]
    chunk = DK
    chunks = q_ref.shape[0] // chunk
    rows = lax.broadcasted_iota(jnp.int32, (chunk, chunk), 0)
    cols = lax.broadcasted_iota(jnp.int32, (chunk, chunk), 1)
    within = rows >= cols
    eye = jnp.where(rows == cols, 1.0, 0.0)
    parts = []
    for h in range(heads):
        for c in range(chunks):
            at = pl.ds(c * chunk, chunk)
            q = q_ref[at, h * DK : (h + 1) * DK].astype(jnp.float32)
            k = k_ref[at, h * DK : (h + 1) * DK].astype(jnp.float32)
            v = v_ref[at, h * DV : (h + 1) * DV].astype(jnp.float32)
            q = unit_rows(q) * DK ** (-0.5)
            k = unit_rows(k)
            d_row = decay_ref[h : h + 1, c * chunk : (c + 1) * chunk]
            b_row = strength_ref[h : h + 1, c * chunk : (c + 1) * chunk]
            d_col = jnp.sum(jnp.where(rows == cols, d_row, 0.0), axis=1, keepdims=True)
            b_col = jnp.sum(jnp.where(rows == cols, b_row, 0.0), axis=1, keepdims=True)
            cum_col = jnp.sum(jnp.where(within, d_row, 0.0), axis=1, keepdims=True)
            cum_row = jnp.sum(jnp.where(rows <= cols, d_col, 0.0), axis=0, keepdims=True)
            last = cum_col[chunk - 1 : chunk, :]
            decayed = jnp.where(within, jnp.exp(jnp.where(within, cum_col - cum_row, 0.0)), 0.0)
            weighted = k * b_col
            lower = jnp.where(
                rows > cols, mm(weighted, k, ((1,), (1,))) * decayed, 0.0
            )
            scores = mm(q, k, ((1,), (1,))) * decayed
            grown = jnp.exp(cum_col)
            rhs = jnp.concatenate([v * b_col, weighted * grown], axis=1)
            parts.append([lower, scores, rhs, q * grown, k * jnp.exp(last - cum_col), jnp.exp(last)])
    inverses = [None] * len(parts)
    span = 1
    while span < chunk:
        mask = (
            (rows // (2 * span) == cols // (2 * span))
            & (rows // span % 2 == 1)
            & (cols // span % 2 == 0)
        )
        for i, part in enumerate(parts):
            edge = jnp.where(mask, part[0], 0.0)
            if span == 1:
                inverses[i] = eye - edge
            else:
                inverses[i] = inverses[i] - mm(mm(inverses[i], edge), inverses[i])
        span *= 2
    solved = [mm(inverse, part[2]) for inverse, part in zip(inverses, parts)]
    yield
    states = [
        jnp.concatenate([jnp.zeros((DK, DV), jnp.float32), eye], axis=1) for _ in range(heads)
    ]
    for c in range(chunks):
        for h in range(heads):
            _, scores, _, queries, keys, retention = parts[h * chunks + c]
            both = solved[h * chunks + c]
            fresh = jnp.concatenate([both[:, :DV], jnp.zeros((chunk, DK), jnp.float32)], axis=1)
            state = states[h]
            updates = fresh - mm(both[:, DV:], state)
            out = mm(queries, state) + mm(scores, updates)
            states[h] = state * retention + mm(keys, updates, ((0,), (0,)))
            at = pl.ds(c * chunk, chunk)
            local_ref[h, at, :] = out[:, :DV]
            proj_ref[h, at, :] = out[:, DV:]
    for h in range(heads):
        end_ref[h] = states[h].astype(end_ref.dtype)
    yield


def delta_kernel(*refs):
    for _ in delta_body(*refs):
        pass


def delta_rule(queries, keys, values, strength, decay_logarithm):
    heads, length = strength.shape
    vmem = pl.BlockSpec(memory_space=pltpu.VMEM)
    f32 = jnp.float32
    return pl.pallas_call(
        delta_kernel,
        out_shape=(
            jax.ShapeDtypeStruct((heads, length, DV), f32),
            jax.ShapeDtypeStruct((heads, length, DK), f32),
            jax.ShapeDtypeStruct((heads, DK, DV + DK), f32),
        ),
        in_specs=[vmem] * 5,
        out_specs=(vmem,) * 3,
        cost_estimate=pl.CostEstimate(
            flops=40 * heads * length * DK * DK * 6, bytes_accessed=4 * 2**20, transcendentals=0
        ),
        compiler_params=pltpu.CompilerParams(vmem_limit_bytes=40 * 2**20),
    )(queries, keys, values, strength, decay_logarithm)


def expert_kernel(x_ref, gate_ref, up_ref, down_ref, out_ref):
    experts, units, width = gate_ref.shape
    x = x_ref[:, :width]
    hidden = []
    for e in range(experts):
        gating = lax.dot_general(
            x, gate_ref[e], (((1,), (1,)), ((), ())), preferred_element_type=jnp.float32
        )
        upward = lax.dot_general(
            x, up_ref[e], (((1,), (1,)), ((), ())), preferred_element_type=jnp.float32
        )
        share = x_ref[:, width + e : width + e + 1].astype(jnp.float32) + x_ref[
            :, width + experts + e : width + experts + e + 1
        ].astype(jnp.float32)
        hidden.append((gating / (1.0 + jnp.exp(-gating)) * upward * share).astype(jnp.bfloat16))
    hidden = jnp.concatenate(hidden, axis=1)
    down = down_ref[...].reshape(experts * units, width)
    out_ref[...] = jnp.dot(hidden, down, preferred_element_type=jnp.float32).astype(jnp.bfloat16)


def expert_layer(rows, gate, up, down, tile):
    count, wide = rows.shape
    experts, units, width = gate.shape
    whole = pl.BlockSpec((experts, units, width), lambda i: (0, 0, 0))
    return pl.pallas_call(
        expert_kernel,
        grid=(count // tile,),
        out_shape=jax.ShapeDtypeStruct((count, width), jnp.bfloat16),
        in_specs=[pl.BlockSpec((tile, wide), lambda i: (i, 0)), whole, whole, whole],
        out_specs=pl.BlockSpec((tile, width), lambda i: (i, 0)),
        cost_estimate=pl.CostEstimate(
            flops=6 * count * experts * units * width,
            bytes_accessed=4 * count * width + 6 * experts * units * width,
            transcendentals=0,
        ),
        compiler_params=pltpu.CompilerParams(vmem_limit_bytes=48 * 2**20),
    )(rows, gate, up, down)


def routing(choice, router, difference, experts, peers):
    tokens = choice.shape[1]
    f32, i32 = jnp.float32, jnp.int32
    ids = choice.astype(f32)
    leading = 1.0 / (1.0 + jnp.exp(-difference))
    parts = (router * leading, router * (1.0 - leading))
    line = lax.broadcasted_iota(i32, (peers * 8, tokens), 0)
    within = lax.rem(line, 8)
    number = jnp.where(within < experts, line // 8 * experts + within, -1).astype(f32)
    first = (lax.broadcasted_iota(i32, (8, tokens), 0) * experts).astype(f32)
    share = jnp.zeros((peers * 8, tokens), f32)
    goes = jnp.zeros((8, tokens), f32)
    for k in range(TOPK):
        named = ids[k : k + 1]
        share = share + jnp.where(named == number, parts[k], 0.0)
        inside = jnp.logical_and(named >= first, named < first + experts)
        goes = jnp.where(inside, 1.0, goes)
    return jnp.concatenate([share, goes], axis=0)


def fused_kernel(*refs):
    arguments, (mixed_ref, expert_ref), rest = refs[:16], refs[16:18], refs[18:]
    copies, rest = rest[:16], rest[16:]
    (
        tokens_ref, scale_ref, choice_ref, router_ref, difference_ref, logit_ref, before_ref,
        rate_ref, extra_ref, q_ref, k_ref, v_ref, gate_ref, up_ref, down_ref, wout_ref,
    ) = copies
    (
        raw, infos, spreads, stage, stage_share, rows, rows_share, hid, res, theirs, back,
        acc, inb, local, proj, attn, states_out, states_in, state, prod, prod_theirs, mixed_in,
        strength_ref, decay_ref, load_sems, ag_s, ag_r, agi_s, agi_r, ep_s, ep_r, eps_s, eps_r, core_s, core_r, cores_s, cores_r,
        pair_s, pair_r, back_s, back_r, rs_s, rs_r, st_s, st_r, pp_s, pp_r, mr_s, mr_r,
    ) = rest
    e, t = lax.axis_index("ep"), lax.axis_index("tp")
    core, z = lax.rem(t, 2), lax.div(t, 2)
    chips, tokens, width = raw.shape
    peers, slots = stage.shape[1], stage.shape[2]
    experts, units, _ = gate_ref.shape
    count = peers * slots
    pieces, part = acc.shape[1], acc.shape[3]
    last = chips - 1
    bf16, f32 = jnp.bfloat16, jnp.float32
    upper = lax.div(z, 2)
    near_end = z + upper * (last - 2 * z)

    def order(i):
        base = (near_end, 1 + 2 * near_end, 3 - 3 * near_end, 2)[i]
        return base + upper * (last - 2 * base)

    swap = (1 - near_end) * (order(2) - order(1))
    returns = (order(1) + swap, order(3), order(2) - swap)
    inner = jnp.logical_and(z >= 1, z <= last - 1)
    outer = jnp.logical_or(z == 0, z == last)
    other = (e, z * 2 + 1 - core)

    def at_chip(chip):
        return (e, chip * 2 + core)

    def at_peer(j):
        return (lax.rem(e + j, peers), t)

    sources = [lax.rem(e + peers - j, peers) for j in range(peers)]

    loads = []
    for i, (src, dst) in enumerate(zip(arguments, copies)):
        copy = pltpu.make_async_copy(src, dst, load_sems.at[i])
        copy.start()
        loads.append(copy)

    barrier = pltpu.get_barrier_semaphore()
    greeted = [at_peer(j) for j in range(1, peers)] + [other]
    greeted += [at_chip(lax.rem(z + h, chips)) for h in range(1, chips)]
    for device in greeted:
        pl.semaphore_signal(barrier, inc=1, device_id=device, device_id_type=MESH)

    started = []

    def send(src, dst, send_sem, recv_sem, device, when=None):
        def make():
            return pltpu.make_async_remote_copy(
                src_ref=src, dst_ref=dst, send_sem=send_sem, recv_sem=recv_sem,
                device_id=device, device_id_type=MESH,
            )

        if when is None:
            make().start()
        else:
            @pl.when(when)
            def _():
                make().start()
        started.append((make, when))

    def arrived(dst, send_sem, recv_sem):
        pltpu.make_async_remote_copy(
            src_ref=dst, dst_ref=dst, send_sem=send_sem, recv_sem=recv_sem,
            device_id=other, device_id_type=MESH,
        ).wait_recv()

    for copy in loads[:5]:
        copy.wait()
    widened = tokens_ref[...].astype(f32)
    raw[z] = (
        widened
        * lax.rsqrt(jnp.mean(widened * widened, axis=-1, keepdims=True) + norm_eps)
        * scale_ref[...]
    ).astype(bf16)
    infos[z] = routing(
        choice_ref[...], router_ref[...], difference_ref[...], experts, peers
    )
    pl.semaphore_wait(barrier, len(greeted))

    step = 1 - 2 * upper

    def share_rows(n, chip, target, when):
        device = at_chip(target)
        send(infos.at[chip], infos.at[chip], agi_s.at[n], agi_r.at[chip], device, when)
        send(raw.at[chip], raw.at[chip], ag_s.at[n], ag_r.at[chip], device, when)

    share_rows(0, z, z + 2 * step, outer)
    share_rows(1, z, z + step, outer)
    share_rows(2, z, z - step, inner)

    def gathered(chip):
        arrived(infos.at[chip], agi_s.at[0], agi_r.at[chip])
        arrived(raw.at[chip], ag_s.at[0], ag_r.at[chip])

    def select(chip):
        info = infos[chip]
        goes = info[peers * 8 : peers * 8 + 8]
        before = lax.broadcasted_iota(jnp.int32, (tokens, tokens), 0) < lax.broadcasted_iota(
            jnp.int32, (tokens, tokens), 1
        )
        rank = jnp.dot(
            goes.astype(bf16), jnp.where(before, 1.0, 0.0).astype(bf16), preferred_element_type=f32
        )
        slot = lax.broadcasted_iota(jnp.int32, (tokens, tokens), 0).astype(f32)
        for g in range(peers):
            hit = jnp.logical_and(slot == rank[g : g + 1], goes[g : g + 1] > 0.5)
            spread = jnp.where(hit, 1.0, 0.0)
            share = mm(info[g * 8 : g * 8 + 8], spread, ((1,), (1,)))
            high = share.astype(bf16)
            low = (share - high.astype(f32)).astype(bf16)
            stage_share[chip, g] = jnp.concatenate([high, low], axis=0)
            spreads[chip, g * slots : (g + 1) * slots] = spread[:slots].astype(bf16)

        def columns(n, carry):
            at = pl.ds(pl.multiple_of(n * 512, 512), 512)
            picked = jnp.dot(spreads[chip], raw[chip, :, at], preferred_element_type=f32)
            stage[chip, :, :, at] = picked.astype(bf16).reshape(peers, slots, 512)
            return carry

        lax.fori_loop(0, width // 512, columns, 0)
        for j in (3, 1, 2):
            target = lax.rem(e + j, peers)
            send(
                stage_share.at[chip, target], rows_share.at[chip, core, e],
                eps_s.at[chip, j], eps_r.at[chip, j], (target, t),
            )
            send(
                stage.at[chip, target], rows.at[chip, core, e],
                ep_s.at[chip, j], ep_r.at[chip, j], (target, t),
            )
        rows[chip, core, e] = stage[chip, e]
        rows_share[chip, core, e] = stage_share[chip, e]

    def pass_on(chip):
        for j in range(1, peers):
            arrived(rows_share.at[chip, core, sources[j]], eps_s.at[chip, j], eps_r.at[chip, j])
            arrived(rows.at[chip, core, sources[j]], ep_s.at[chip, j], ep_r.at[chip, j])
        send(
            rows_share.at[chip, core], rows_share.at[chip, core],
            cores_s.at[chip], cores_r.at[chip], other,
        )
        send(rows.at[chip, core], rows.at[chip, core], core_s.at[chip], core_r.at[chip], other)

    def produce(chip):
        arrived(rows_share.at[chip, 1 - core], cores_s.at[chip], cores_r.at[chip])
        arrived(rows.at[chip, 1 - core], core_s.at[chip], core_r.at[chip])
        unit = lax.broadcasted_iota(jnp.int32, (16, 2 * units), 1) // units
        which = lax.rem(lax.broadcasted_iota(jnp.int32, (16, 2 * units), 0), 8)

        def expert_pair(n, carry):
            pick = jnp.where(which == unit + 2 * n, 1.0, 0.0).astype(bf16)
            share = [
                lax.dot_general(
                    rows_share[chip, c, p], pick, (((0,), (0,)), ((), ())),
                    preferred_element_type=f32,
                )[:slots]
                for c in range(2)
                for p in range(peers)
            ]
            share = jnp.concatenate(share, axis=0)
            x = rows[chip].reshape(2 * count, width)
            gating = lax.dot_general(
                x, gate_ref[pl.ds(2 * n, 2)].reshape(2 * units, width),
                (((1,), (1,)), ((), ())), preferred_element_type=f32,
            )
            upward = lax.dot_general(
                x, up_ref[pl.ds(2 * n, 2)].reshape(2 * units, width),
                (((1,), (1,)), ((), ())), preferred_element_type=f32,
            )
            at = pl.ds(pl.multiple_of(n * 2 * units, 2 * units), 2 * units)
            hid[:, at] = (gating / (1.0 + jnp.exp(-gating)) * upward * share).astype(bf16)
            return carry

        lax.fori_loop(0, experts // 2, expert_pair, 0)

        def columns(n, carry):
            at = pl.ds(pl.multiple_of(n * 512, 512), 512)
            down = down_ref[:, :, at].reshape(experts * units, 512)
            made = jnp.dot(hid[...], down, preferred_element_type=f32)
            res[chip, :, :, :, at] = made.astype(bf16).reshape(2, peers, slots, 512)
            return carry

        lax.fori_loop(0, width // 512, columns, 0)
        send(res.at[chip, 1 - core], theirs.at[chip], pair_s.at[chip], pair_r.at[chip], other)

    def give_back(chip):
        arrived(theirs.at[chip], pair_s.at[chip], pair_r.at[chip])
        res[chip, core] = (res[chip, core].astype(f32) + theirs[chip].astype(f32)).astype(bf16)
        for j in (3, 1, 2):
            target = lax.rem(e + j, peers)
            send(
                res.at[chip, core, target], back.at[chip, e],
                back_s.at[chip, j], back_r.at[chip, j], (target, t),
            )
        back[chip, e] = res[chip, core, e]

    def unselect(chip):
        for j in range(1, peers):
            arrived(back.at[chip, sources[j]], back_s.at[chip, j], back_r.at[chip, j])
        for h in range(pieces):
            acc[chip, h] = lax.dot_general(
                spreads[chip],
                back[chip, :, :, h * part : (h + 1) * part].reshape(count, part),
                (((0,), (0,)), ((), ())), preferred_element_type=f32,
            ).astype(bf16)

    def add_from(total, piece, send_sem, recv_sem):
        @pl.when(inner)
        def _():
            arrived(piece, send_sem, recv_sem)
            total[...] = (total[...].astype(f32) + piece[...].astype(f32)).astype(bf16)

    def forward(chip, joins, which, when=None):
        device = at_chip(z + step + near_end * (chip - z - step))
        slot = chip + (near_end * (chips - chip) if joins else 0)
        for h in which:
            if joins:
                add_from(acc.at[chip, h], inb.at[chip, h], rs_s.at[chip, h], rs_r.at[chip, h])
            send(
                acc.at[chip, h], inb.at[slot, h], rs_s.at[chip, h], rs_r.at[slot, h], device, when
            )

    def keep_order():
        def body(i, carry):
            state[0] = jnp.zeros_like(state[0])
            return carry

        lax.fori_loop(0, t // (4 * chips), body, 0)

    def finish(first, parts, sems, out, at):
        total = first[...].astype(f32)
        for piece, sem in zip(parts, sems[1:]):
            arrived(piece, sems[0], sem)
            total = total + piece[...].astype(f32)
        out[:, at] = total.astype(bf16)

    heads = local.shape[0]

    def send_states():
        for j in range(1, peers):
            send(states_out, states_in.at[j], st_s.at[j], st_r.at[j], at_peer(j), e < peers - j)

    def project():
        state[...] = jnp.zeros_like(state)
        for j in range(peers - 1, 0, -1):
            @pl.when(e >= j)
            def _():
                arrived(states_in.at[j], st_s.at[j], st_r.at[j])
                for h in range(heads):
                    piece = states_in[j, h].astype(f32)
                    state[h] = piece[:, :DV] + mm(piece[:, DV:], state[h])
        for h in range(heads):
            attn[:, h * DV : (h + 1) * DV] = (local[h] + mm(proj[h], state[h])).astype(bf16)
        loads[15].wait()
        share = prod.shape[2]

        def columns(n, carry):
            at = pl.ds(pl.multiple_of(n * 512, 512), 512)
            made = jnp.dot(attn[...], wout_ref[:, at], preferred_element_type=f32)
            made = made.astype(bf16).reshape(chips, 2, share, 512)
            for c in range(2):
                prod[c, :, :, at] = made[:, c]
            return carry

        lax.fori_loop(0, width // 512, columns, 0)
        send(prod.at[1 - core], prod_theirs, pp_s, pp_r, other)

    def join_mixed():
        arrived(prod_theirs, pp_s, pp_r)
        prod[core] = (prod[core].astype(f32) + prod_theirs[...].astype(f32)).astype(bf16)

    def send_mixed(chip, slot, target, when):
        send(
            prod.at[core, chip], mixed_in.at[slot],
            mr_s.at[chip], mr_r.at[slot], at_chip(target), when,
        )

    def start_mixed():
        for n in (3, 2, 1):
            send_mixed(z + n * step, z + n * step, z + step, outer)
        send_mixed(z - step, z - step, z - step, inner)

    def pass_mixed():
        for n in (2, 1):
            chip = z + n * step

            @pl.when(inner)
            def _():
                arrived(mixed_in.at[chip], mr_s.at[chip], mr_r.at[chip])
                prod[core, chip] = (
                    prod[core, chip].astype(f32) + mixed_in[chip].astype(f32)
                ).astype(bf16)

            send_mixed(chip, chips, chip, inner)

    select(order(0))
    keep_order()
    for copy in loads[5:12]:
        copy.wait()
    strength_ref[...] = 1.0 / (1.0 + jnp.exp(-logit_ref[...].astype(f32)))
    before = before_ref[...].astype(f32)
    growth = jnp.maximum(before, 0.0) + jnp.log1p(jnp.exp(-jnp.abs(before)))
    for h in range(heads):
        decay_ref[h : h + 1] = (
            -jnp.exp(rate_ref[:, h : h + 1]) * growth[h : h + 1] + extra_ref[h : h + 1]
        )
    delta = delta_body(q_ref, k_ref, v_ref, strength_ref, decay_ref, local, proj, states_out)
    next(delta)
    keep_order()
    gathered(order(1))
    share_rows(3, order(1), z - step, inner)
    share_rows(1, z, z + step, inner)
    select(order(1))
    keep_order()
    next(delta)
    keep_order()
    send_states()
    pass_on(order(0))
    keep_order()
    for copy in loads[12:15]:
        copy.wait()
    produce(order(0))
    keep_order()
    gathered(order(2))
    share_rows(0, z, z + 2 * step, inner)
    select(order(2))
    keep_order()
    pass_on(order(1))
    keep_order()
    produce(order(1))
    keep_order()
    gathered(order(3))
    select(order(3))
    keep_order()
    project()
    keep_order()
    pass_on(order(2))
    keep_order()
    produce(order(2))
    keep_order()
    join_mixed()
    start_mixed()
    keep_order()
    give_back(returns[0])
    keep_order()
    pass_on(order(3))
    keep_order()
    produce(order(3))
    keep_order()
    give_back(returns[1])
    keep_order()
    give_back(returns[2])
    keep_order()
    give_back(order(0))
    keep_order()
    pass_mixed()
    keep_order()
    unselect(returns[0])
    keep_order()
    forward(returns[0], True, range(pieces))
    keep_order()
    unselect(returns[1])
    keep_order()
    forward(returns[1], False, range(pieces), outer)
    forward(returns[1], True, range(pieces // 2), inner)
    keep_order()
    finish(
        prod.at[core, z], (mixed_in.at[z], mixed_in.at[chips]),
        (mr_s.at[0], mr_r.at[z], mr_r.at[chips]), mixed_ref, slice(0, width),
    )
    unselect(returns[2])
    keep_order()
    forward(returns[2], False, range(pieces))
    forward(returns[1], True, range(pieces // 2, pieces), inner)
    keep_order()
    unselect(order(0))
    keep_order()
    for h in range(pieces):
        finish(
            acc.at[z, h], (inb.at[z, h], inb.at[chips, h]),
            (rs_s.at[0, h], rs_r.at[z, h], rs_r.at[chips, h]),
            expert_ref, slice(h * part, (h + 1) * part),
        )
    for make, when in started:
        if when is None:
            make().wait_send()
        else:
            @pl.when(when)
            def _():
                make().wait_send()


def fused(
    tokens, scale, choice, router, difference, logit, before, rate, extra,
    queries, keys, values, gate, up, down, out_weight, slots,
):
    experts, units, width = gate.shape
    count, peers, chips, pieces = tokens.shape[0], lax.axis_size("ep"), RING, 4
    heads, length = extra.shape
    part = width // pieces
    share = length // (2 * chips)
    bf16, f32 = jnp.bfloat16, jnp.float32
    vmem = pl.BlockSpec(memory_space=pltpu.VMEM)
    anywhere = pl.BlockSpec(memory_space=pl.ANY)
    dma = pltpu.SemaphoreType.DMA

    def room(*shape, dtype=bf16):
        return pltpu.VMEM(shape, dtype)

    arguments = [
        tokens, scale, choice, router, difference, logit, before, rate, extra,
        queries, keys, values, gate, up, down, out_weight,
    ]
    return pl.pallas_call(
        fused_kernel,
        out_shape=(
            jax.ShapeDtypeStruct((share, width), bf16),
            jax.ShapeDtypeStruct((count, width), bf16),
        ),
        in_specs=[anywhere] * len(arguments),
        out_specs=(vmem, vmem),
        scratch_shapes=[room(*a.shape, dtype=a.dtype) for a in arguments]
        + [
            room(chips, count, width),
            room(chips, (peers + 1) * 8, count, dtype=f32),
            room(chips, peers * slots, count),
            room(chips, peers, slots, width),
            room(chips, peers, 16, count),
            room(chips, 2, peers, slots, width),
            room(chips, 2, peers, 16, count),
            room(2 * peers * slots, experts * units),
            room(chips, 2, peers, slots, width),
            room(chips, peers, slots, width),
            room(chips, peers, slots, width),
            room(chips, pieces, count, part),
            room(chips + 1, pieces, count, part),
            room(heads, length, DV, dtype=f32),
            room(heads, length, DK, dtype=f32),
            room(length, heads * DV),
            room(heads, DK, DV + DK),
            room(peers, heads, DK, DV + DK),
            room(heads, DK, DV, dtype=f32),
            room(2, chips, share, width),
            room(chips, share, width),
            room(chips + 1, share, width),
            room(heads, length, dtype=f32),
            room(heads, length, dtype=f32),
            dma((len(arguments),)),
            dma((5,)), dma((chips,)), dma((5,)), dma((chips,)),
            dma((chips, peers)), dma((chips, peers)), dma((chips, peers)), dma((chips, peers)),
            dma((chips,)), dma((chips,)), dma((chips,)), dma((chips,)),
            dma((chips,)), dma((chips,)),
            dma((chips, peers)), dma((chips, peers)),
            dma((chips, pieces)), dma((chips + 1, pieces)),
            dma((peers,)), dma((peers,)), dma, dma,
            dma((chips,)), dma((chips + 1,)),
        ],
        cost_estimate=pl.CostEstimate(
            flops=12 * chips * peers * slots * experts * units * width,
            bytes_accessed=8 * experts * units * width,
            transcendentals=0,
        ),
        compiler_params=pltpu.CompilerParams(
            collective_id=0, has_side_effects=True, vmem_limit_bytes=63 * 2**20
        ),
    )(*arguments)


def by_tokens(normed, choice, mixing, gate, up, down, slots, after):
    ep_count = lax.axis_size("ep")
    local_experts = gate.shape[0]
    tokens, width = normed.shape
    bf16 = jnp.bfloat16
    f32 = jnp.float32
    named = choice[:, :, None] == jnp.arange(ep_count * local_experts, dtype=jnp.int32)
    share = jnp.sum(jnp.where(named, mixing[:, :, None], 0.0), axis=1)
    goes = jnp.any(named, axis=1).reshape(tokens, ep_count, local_experts).any(axis=-1)
    earlier = jnp.tril(jnp.ones((tokens, tokens), bf16), -1)
    rank = jnp.dot(earlier, goes.astype(bf16), preferred_element_type=f32)
    spread = goes[:, :, None] & (rank[:, :, None] == jnp.arange(slots, dtype=f32))
    spread = spread.astype(bf16)
    high = share.astype(bf16)
    low = (share - high.astype(f32)).astype(bf16)
    sent = jnp.einsum("tes,td->esd", spread, normed, preferred_element_type=f32).astype(bf16)
    extra = jnp.concatenate(
        [
            high.reshape(tokens, ep_count, local_experts),
            low.reshape(tokens, ep_count, local_experts),
        ],
        axis=-1,
    )
    extra = jnp.einsum("tes,tex->esx", spread, extra, preferred_element_type=f32).astype(bf16)
    pad = -extra.shape[-1] % 128
    extra = jnp.pad(extra, ((0, 0), (0, 0), (0, pad)))
    outgoing = jnp.concatenate([sent, extra], axis=-1)
    arrived = lax.all_to_all(outgoing, "ep", split_axis=0, concat_axis=0, tiled=True)
    arrived = arrived.reshape(ep_count * slots, -1)
    everyone = lax.all_gather(arrived, "tp", axis=0, tiled=True)
    produced = expert_layer(everyone, gate, up, down, arrived.shape[0])
    summed = lax.psum_scatter(produced, "tp", scatter_dimension=0, tiled=True)
    returned = lax.all_to_all(
        summed.reshape(ep_count, slots, width), "ep", split_axis=0, concat_axis=0, tiled=True
    )
    combined = jnp.einsum("tes,esd->td", spread, returned, preferred_element_type=f32)
    return combined.astype(bf16), after


def by_weights(normed, expert_choice_index, mixing, gate, up, down):
    own_tokens, width_model = normed.shape
    ep_count = lax.axis_size("ep")
    local_experts = gate.shape[0]
    experts = local_experts * ep_count
    flat_ids = expert_choice_index.reshape(-1)
    one_hot = (flat_ids[:, None] == jnp.arange(experts, dtype=jnp.int32)[None, :]).astype(jnp.int32)
    slot_rank = jnp.sum((jnp.cumsum(one_hot, axis=0) - one_hot) * one_hot, axis=1)
    slot_index = flat_ids * CAP + slot_rank
    copy_token = jnp.arange(flat_ids.shape[0], dtype=jnp.int32) // TOPK
    slot_token = jnp.full((experts * CAP,), own_tokens, jnp.int32).at[slot_index].set(copy_token)
    outgoing = jnp.take(normed, slot_token, axis=0, mode="fill", fill_value=0).reshape(
        ep_count, local_experts, CAP, width_model
    )
    arrived = lax.all_to_all(outgoing, "ep", split_axis=0, concat_axis=0, tiled=True)
    gate_piece = lax.all_gather(gate, "tp", axis=1, tiled=True)
    up_piece = lax.all_gather(up, "tp", axis=1, tiled=True)
    down_piece = lax.all_gather(down, "tp", axis=1, tiled=True)
    gating = jnp.einsum("secd,efd->secf", arrived, gate_piece, preferred_element_type=jnp.float32)
    upward = jnp.einsum("secd,efd->secf", arrived, up_piece, preferred_element_type=jnp.float32)
    hidden = (jax.nn.silu(gating) * upward).astype(jnp.bfloat16)
    produced = jnp.einsum("secf,efd->secd", hidden, down_piece, preferred_element_type=jnp.float32)
    returned = lax.all_to_all(
        produced.astype(jnp.bfloat16), "ep", split_axis=0, concat_axis=0, tiled=True
    )
    flat_results = returned.reshape(experts * CAP, width_model)
    picked = (
        jnp.take(flat_results, slot_index, axis=0)
        .reshape(own_tokens, TOPK, width_model)
        .astype(jnp.float32)
    )
    return jnp.sum(mixing[..., None] * picked, axis=1).astype(jnp.bfloat16)


def shards(
    query_heads_rows,
    key_heads_rows,
    value_heads_rows,
    write_strength_logit,
    decay_preactivation,
    head_decay_logarithm,
    extra_log_decay,
    output_weight,
    second_batch_tokens,
    expert_norm_scale,
    expert_choice_index,
    group_router_weight,
    expert_logit_difference,
    expert_gate_weight,
    expert_up_weight,
    expert_down_weight,
):
    length = query_heads_rows.shape[0]
    local_heads = head_decay_logarithm.shape[0]
    strength = jax.nn.sigmoid(write_strength_logit.astype(jnp.float32))
    decay_logarithm = (
        -jnp.exp(head_decay_logarithm)[:, None]
        * jax.nn.softplus(decay_preactivation.astype(jnp.float32))
        + extra_log_decay
    )
    leading = jax.nn.sigmoid(expert_logit_difference)
    mixing = group_router_weight[:, None] * jnp.stack([leading, 1.0 - leading], axis=-1)
    local_experts, local_units, width = expert_gate_weight.shape
    own_tokens = second_batch_tokens.shape[0]
    ep_count, tp_count = lax.axis_size("ep"), lax.axis_size("tp")
    named_both = TOPK if local_experts % EPG == 0 else 1
    slots = min(own_tokens, local_experts * CAP // named_both)
    weights = (expert_gate_weight, expert_up_weight, expert_down_weight)
    if (
        (ep_count, tp_count) == (RING, 2 * RING)
        and named_both == TOPK
        and own_tokens == DK
        and local_experts * local_units == width // RING
    ):
        return fused(
            second_batch_tokens, expert_norm_scale.reshape(1, width), expert_choice_index.T,
            group_router_weight.reshape(1, own_tokens),
            expert_logit_difference.reshape(1, own_tokens),
            write_strength_logit, decay_preactivation,
            head_decay_logarithm.reshape(1, local_heads), extra_log_decay,
            query_heads_rows, key_heads_rows, value_heads_rows, *weights, output_weight, slots,
        )
    local_output, projection_matrix, end_memory = delta_rule(
        query_heads_rows, key_heads_rows, value_heads_rows, strength, decay_logarithm
    )
    incoming_rows = incoming(end_memory, "ep")
    attention_result = local_output + jnp.einsum(
        "hpg,hgd->hpd", projection_matrix, incoming_rows, precision=precise_setting
    )
    attn_rows = (
        attention_result.transpose(1, 0, 2)
        .reshape(length, local_heads * DV)
        .astype(jnp.bfloat16)
    )
    product = jnp.dot(attn_rows, output_weight, preferred_element_type=jnp.float32)
    product = product.astype(jnp.bfloat16)
    widened = second_batch_tokens.astype(jnp.float32)
    normed = (
        widened
        * lax.rsqrt(jnp.mean(widened * widened, axis=-1, keepdims=True) + norm_eps)
        * expert_norm_scale
    ).astype(jnp.bfloat16)
    if 2 * tp_count * ep_count * slots < 3 * local_experts * local_units * tp_count:
        expert_out, product = by_tokens(
            normed, expert_choice_index, mixing, *weights, slots, product
        )
    else:
        expert_out = by_weights(normed, expert_choice_index, mixing, *weights)
    summed = lax.psum_scatter(product, "tp", scatter_dimension=0, tiled=True)
    return (summed, expert_out)


def solution(mesh):
    in_specs = (
        P("ep", "tp"),
        P("ep", "tp"),
        P("ep", "tp"),
        P("tp", "ep"),
        P("tp", "ep"),
        P("tp"),
        P("tp", "ep"),
        P("tp", None),
        P(("ep", "tp"), None),
        P(),
        P(("ep", "tp"), None),
        P(("ep", "tp")),
        P(("ep", "tp")),
        P("ep", "tp", None),
        P("ep", "tp", None),
        P("ep", "tp", None),
    )
    out_specs = (P(("ep", "tp"), None), P(("ep", "tp"), None))
    return jax.shard_map(shards, mesh=mesh, in_specs=in_specs, out_specs=out_specs, check_vma=False)
```

```python
import functools

import jax
import jax.numpy as jnp
from jax import lax
from jax.experimental import pallas as pl
from jax.experimental.pallas import tpu as pltpu
from jax.sharding import PartitionSpec as P

DK = 128
DV = 128
CAP = 32
RING = 4
MESH = pl.DeviceIdType.MESH
EPG = 4
TOPK = 2


precise_setting = lax.Precision.HIGHEST
norm_eps = 1e-06


def incoming(end_memory, axis):
    count, mine = (lax.axis_size(axis), lax.axis_index(axis))
    pieces = lax.all_gather(end_memory, axis)
    state = jnp.zeros(end_memory.shape[:-1] + (DV,), jnp.float32)
    for position in range(count - 1):
        end, transfer = pieces[position, ..., :DV], pieces[position, ..., DV:]
        longer = end + jnp.einsum("hij,hjv->hiv", transfer, state, precision=precise_setting)
        state = jnp.where(position < mine, longer, state)
    return state


def unit_rows(matrix):
    return matrix * lax.rsqrt(jnp.sum(matrix * matrix, axis=-1, keepdims=True) + norm_eps)


def mm(a, b, dims=((1,), (0,))):
    return lax.dot_general(
        a, b, (dims, ((), ())), precision=precise_setting, preferred_element_type=jnp.float32
    )


def delta_body(q_ref, k_ref, v_ref, strength_ref, decay_ref, local_ref, proj_ref, end_ref):
    heads = strength_ref.shape[0]
    chunk = DK
    chunks = q_ref.shape[0] // chunk
    rows = lax.broadcasted_iota(jnp.int32, (chunk, chunk), 0)
    cols = lax.broadcasted_iota(jnp.int32, (chunk, chunk), 1)
    within = rows >= cols
    eye = jnp.where(rows == cols, 1.0, 0.0)
    parts = []
    for h in range(heads):
        for c in range(chunks):
            at = pl.ds(c * chunk, chunk)
            q = q_ref[at, h * DK : (h + 1) * DK].astype(jnp.float32)
            k = k_ref[at, h * DK : (h + 1) * DK].astype(jnp.float32)
            v = v_ref[at, h * DV : (h + 1) * DV].astype(jnp.float32)
            q = unit_rows(q) * DK ** (-0.5)
            k = unit_rows(k)
            d_row = decay_ref[h : h + 1, c * chunk : (c + 1) * chunk]
            b_row = strength_ref[h : h + 1, c * chunk : (c + 1) * chunk]
            d_col = jnp.sum(jnp.where(rows == cols, d_row, 0.0), axis=1, keepdims=True)
            b_col = jnp.sum(jnp.where(rows == cols, b_row, 0.0), axis=1, keepdims=True)
            cum_col = jnp.sum(jnp.where(within, d_row, 0.0), axis=1, keepdims=True)
            cum_row = jnp.sum(jnp.where(rows <= cols, d_col, 0.0), axis=0, keepdims=True)
            last = cum_col[chunk - 1 : chunk, :]
            decayed = jnp.where(within, jnp.exp(jnp.where(within, cum_col - cum_row, 0.0)), 0.0)
            weighted = k * b_col
            lower = jnp.where(
                rows > cols, mm(weighted, k, ((1,), (1,))) * decayed, 0.0
            )
            scores = mm(q, k, ((1,), (1,))) * decayed
            grown = jnp.exp(cum_col)
            rhs = jnp.concatenate([v * b_col, weighted * grown], axis=1)
            parts.append([lower, scores, rhs, q * grown, k * jnp.exp(last - cum_col), jnp.exp(last)])
    inverses = [None] * len(parts)
    span = 1
    while span < chunk:
        mask = (
            (rows // (2 * span) == cols // (2 * span))
            & (rows // span % 2 == 1)
            & (cols // span % 2 == 0)
        )
        for i, part in enumerate(parts):
            edge = jnp.where(mask, part[0], 0.0)
            if span == 1:
                inverses[i] = eye - edge
            else:
                inverses[i] = inverses[i] - mm(mm(inverses[i], edge), inverses[i])
        span *= 2
    solved = [mm(inverse, part[2]) for inverse, part in zip(inverses, parts)]
    yield
    states = [
        jnp.concatenate([jnp.zeros((DK, DV), jnp.float32), eye], axis=1) for _ in range(heads)
    ]
    for c in range(chunks):
        for h in range(heads):
            _, scores, _, queries, keys, retention = parts[h * chunks + c]
            both = solved[h * chunks + c]
            fresh = jnp.concatenate([both[:, :DV], jnp.zeros((chunk, DK), jnp.float32)], axis=1)
            state = states[h]
            updates = fresh - mm(both[:, DV:], state)
            out = mm(queries, state) + mm(scores, updates)
            states[h] = state * retention + mm(keys, updates, ((0,), (0,)))
            at = pl.ds(c * chunk, chunk)
            local_ref[h, at, :] = out[:, :DV]
            proj_ref[h, at, :] = out[:, DV:]
    for h in range(heads):
        end_ref[h] = states[h].astype(end_ref.dtype)
    yield


def delta_kernel(*refs):
    for _ in delta_body(*refs):
        pass


def delta_rule(queries, keys, values, strength, decay_logarithm):
    heads, length = strength.shape
    vmem = pl.BlockSpec(memory_space=pltpu.VMEM)
    f32 = jnp.float32
    return pl.pallas_call(
        delta_kernel,
        out_shape=(
            jax.ShapeDtypeStruct((heads, length, DV), f32),
            jax.ShapeDtypeStruct((heads, length, DK), f32),
            jax.ShapeDtypeStruct((heads, DK, DV + DK), f32),
        ),
        in_specs=[vmem] * 5,
        out_specs=(vmem,) * 3,
        cost_estimate=pl.CostEstimate(
            flops=40 * heads * length * DK * DK * 6, bytes_accessed=4 * 2**20, transcendentals=0
        ),
        compiler_params=pltpu.CompilerParams(vmem_limit_bytes=40 * 2**20),
    )(queries, keys, values, strength, decay_logarithm)


def expert_kernel(x_ref, gate_ref, up_ref, down_ref, out_ref):
    experts, units, width = gate_ref.shape
    x = x_ref[:, :width]
    hidden = []
    for e in range(experts):
        gating = lax.dot_general(
            x, gate_ref[e], (((1,), (1,)), ((), ())), preferred_element_type=jnp.float32
        )
        upward = lax.dot_general(
            x, up_ref[e], (((1,), (1,)), ((), ())), preferred_element_type=jnp.float32
        )
        share = x_ref[:, width + e : width + e + 1].astype(jnp.float32) + x_ref[
            :, width + experts + e : width + experts + e + 1
        ].astype(jnp.float32)
        hidden.append((gating / (1.0 + jnp.exp(-gating)) * upward * share).astype(jnp.bfloat16))
    hidden = jnp.concatenate(hidden, axis=1)
    down = down_ref[...].reshape(experts * units, width)
    out_ref[...] = jnp.dot(hidden, down, preferred_element_type=jnp.float32).astype(jnp.bfloat16)


def expert_layer(rows, gate, up, down, tile):
    count, wide = rows.shape
    experts, units, width = gate.shape
    whole = pl.BlockSpec((experts, units, width), lambda i: (0, 0, 0))
    return pl.pallas_call(
        expert_kernel,
        grid=(count // tile,),
        out_shape=jax.ShapeDtypeStruct((count, width), jnp.bfloat16),
        in_specs=[pl.BlockSpec((tile, wide), lambda i: (i, 0)), whole, whole, whole],
        out_specs=pl.BlockSpec((tile, width), lambda i: (i, 0)),
        cost_estimate=pl.CostEstimate(
            flops=6 * count * experts * units * width,
            bytes_accessed=4 * count * width + 6 * experts * units * width,
            transcendentals=0,
        ),
        compiler_params=pltpu.CompilerParams(vmem_limit_bytes=48 * 2**20),
    )(rows, gate, up, down)


def routing(choice, router, difference, experts, peers):
    tokens = choice.shape[1]
    f32, i32 = jnp.float32, jnp.int32
    ids = choice.astype(f32)
    leading = 1.0 / (1.0 + jnp.exp(-difference))
    parts = (router * leading, router * (1.0 - leading))
    line = lax.broadcasted_iota(i32, (peers * 8, tokens), 0)
    within = lax.rem(line, 8)
    number = jnp.where(within < experts, line // 8 * experts + within, -1).astype(f32)
    first = (lax.broadcasted_iota(i32, (8, tokens), 0) * experts).astype(f32)
    share = jnp.zeros((peers * 8, tokens), f32)
    goes = jnp.zeros((8, tokens), f32)
    for k in range(TOPK):
        named = ids[k : k + 1]
        share = share + jnp.where(named == number, parts[k], 0.0)
        inside = jnp.logical_and(named >= first, named < first + experts)
        goes = jnp.where(inside, 1.0, goes)
    return jnp.concatenate([share, goes], axis=0)


def fused_kernel(*refs):
    arguments, (mixed_hbm, expert_hbm), rest = refs[:16], refs[16:18], refs[18:]
    copies, rest = rest[:16], rest[16:]
    (
        tokens_ref, scale_ref, choice_ref, router_ref, difference_ref, logit_ref, before_ref,
        rate_ref, extra_ref, q_ref, k_ref, v_ref, gate_ref, up_ref, down_ref, wout_ref,
    ) = copies
    (
        raw, infos, spreads, stage, stage_share, rows, rows_share, hid, res, theirs, back,
        acc, inb, local, proj, attn, states_out, states_in, state, prod, prod_theirs, mixed_in,
        strength_ref, decay_ref, mixed_ref, expert_ref, load_sems, out_sems, ag_s, ag_r, agi_s, agi_r, ep_s, ep_r, eps_s, eps_r, core_s, core_r, cores_s, cores_r,
        pair_s, pair_r, back_s, back_r, rs_s, rs_r, st_s, st_r, pp_s, pp_r, mr_s, mr_r,
    ) = rest
    e, t = lax.axis_index("ep"), lax.axis_index("tp")
    core, z = lax.rem(t, 2), lax.div(t, 2)
    chips, tokens, width = raw.shape
    peers, slots = stage.shape[1], stage.shape[2]
    experts, units, _ = gate_ref.shape
    count = peers * slots
    pieces, part = acc.shape[1], acc.shape[3]
    last = chips - 1
    bf16, f32 = jnp.bfloat16, jnp.float32
    upper = lax.div(z, 2)
    near_end = z + upper * (last - 2 * z)

    def order(i):
        base = (near_end, 1 + 2 * near_end, 3 - 3 * near_end, 2)[i]
        return base + upper * (last - 2 * base)

    swap = (1 - near_end) * (order(2) - order(1))
    returns = (order(1) + swap, order(3), order(2) - swap)
    inner = jnp.logical_and(z >= 1, z <= last - 1)
    outer = jnp.logical_or(z == 0, z == last)
    other = (e, z * 2 + 1 - core)

    def at_chip(chip):
        return (e, chip * 2 + core)

    def at_peer(j):
        return (lax.rem(e + j, peers), t)

    sources = [lax.rem(e + peers - j, peers) for j in range(peers)]

    loads = []
    for i, (src, dst) in enumerate(zip(arguments, copies)):
        copy = pltpu.make_async_copy(src, dst, load_sems.at[i])
        copy.start()
        loads.append(copy)

    barrier = pltpu.get_barrier_semaphore()
    greeted = [at_peer(j) for j in range(1, peers)] + [other]
    greeted += [at_chip(lax.rem(z + h, chips)) for h in range(1, chips)]
    for device in greeted:
        pl.semaphore_signal(barrier, inc=1, device_id=device, device_id_type=MESH)

    started = []

    def send(src, dst, send_sem, recv_sem, device, when=None):
        def make():
            return pltpu.make_async_remote_copy(
                src_ref=src, dst_ref=dst, send_sem=send_sem, recv_sem=recv_sem,
                device_id=device, device_id_type=MESH,
            )

        if when is None:
            make().start()
        else:
            @pl.when(when)
            def _():
                make().start()
        started.append((make, when))

    def arrived(dst, send_sem, recv_sem):
        pltpu.make_async_remote_copy(
            src_ref=dst, dst_ref=dst, send_sem=send_sem, recv_sem=recv_sem,
            device_id=other, device_id_type=MESH,
        ).wait_recv()

    for copy in loads[:5]:
        copy.wait()
    widened = tokens_ref[...].astype(f32)
    raw[z] = (
        widened
        * lax.rsqrt(jnp.mean(widened * widened, axis=-1, keepdims=True) + norm_eps)
        * scale_ref[...]
    ).astype(bf16)
    infos[z] = routing(
        choice_ref[...], router_ref[...], difference_ref[...], experts, peers
    )
    pl.semaphore_wait(barrier, len(greeted))

    step = 1 - 2 * upper

    def share_rows(n, chip, target, when):
        device = at_chip(target)
        send(infos.at[chip], infos.at[chip], agi_s.at[n], agi_r.at[chip], device, when)
        send(raw.at[chip], raw.at[chip], ag_s.at[n], ag_r.at[chip], device, when)

    share_rows(0, z, z + 2 * step, outer)
    share_rows(1, z, z + step, outer)
    share_rows(2, z, z - step, inner)

    def gathered(chip):
        arrived(infos.at[chip], agi_s.at[0], agi_r.at[chip])
        arrived(raw.at[chip], ag_s.at[0], ag_r.at[chip])

    def select(chip):
        info = infos[chip]
        goes = info[peers * 8 : peers * 8 + 8]
        before = lax.broadcasted_iota(jnp.int32, (tokens, tokens), 0) < lax.broadcasted_iota(
            jnp.int32, (tokens, tokens), 1
        )
        rank = jnp.dot(
            goes.astype(bf16), jnp.where(before, 1.0, 0.0).astype(bf16), preferred_element_type=f32
        )
        slot = lax.broadcasted_iota(jnp.int32, (tokens, tokens), 0).astype(f32)
        for g in range(peers):
            hit = jnp.logical_and(slot == rank[g : g + 1], goes[g : g + 1] > 0.5)
            spread = jnp.where(hit, 1.0, 0.0)
            share = mm(info[g * 8 : g * 8 + 8], spread, ((1,), (1,)))
            high = share.astype(bf16)
            low = (share - high.astype(f32)).astype(bf16)
            stage_share[chip, g] = jnp.concatenate([high, low], axis=0)
            spreads[chip, g * slots : (g + 1) * slots] = spread[:slots].astype(bf16)

        def columns(n, carry):
            at = pl.ds(pl.multiple_of(n * 512, 512), 512)
            picked = jnp.dot(spreads[chip], raw[chip, :, at], preferred_element_type=f32)
            stage[chip, :, :, at] = picked.astype(bf16).reshape(peers, slots, 512)
            return carry

        lax.fori_loop(0, width // 512, columns, 0)
        for j in (3, 1, 2):
            target = lax.rem(e + j, peers)
            send(
                stage_share.at[chip, target], rows_share.at[chip, core, e],
                eps_s.at[chip, j], eps_r.at[chip, j], (target, t),
            )
            send(
                stage.at[chip, target], rows.at[chip, core, e],
                ep_s.at[chip, j], ep_r.at[chip, j], (target, t),
            )
        rows[chip, core, e] = stage[chip, e]
        rows_share[chip, core, e] = stage_share[chip, e]

    def pass_on(chip):
        for j in range(1, peers):
            arrived(rows_share.at[chip, core, sources[j]], eps_s.at[chip, j], eps_r.at[chip, j])
            arrived(rows.at[chip, core, sources[j]], ep_s.at[chip, j], ep_r.at[chip, j])
        send(
            rows_share.at[chip, core], rows_share.at[chip, core],
            cores_s.at[chip], cores_r.at[chip], other,
        )
        send(rows.at[chip, core], rows.at[chip, core], core_s.at[chip], core_r.at[chip], other)

    def produce(chip):
        arrived(rows_share.at[chip, 1 - core], cores_s.at[chip], cores_r.at[chip])
        arrived(rows.at[chip, 1 - core], core_s.at[chip], core_r.at[chip])
        unit = lax.broadcasted_iota(jnp.int32, (16, 2 * units), 1) // units
        which = lax.rem(lax.broadcasted_iota(jnp.int32, (16, 2 * units), 0), 8)

        def expert_pair(n, carry):
            pick = jnp.where(which == unit + 2 * n, 1.0, 0.0).astype(bf16)
            share = [
                lax.dot_general(
                    rows_share[chip, c, p], pick, (((0,), (0,)), ((), ())),
                    preferred_element_type=f32,
                )[:slots]
                for c in range(2)
                for p in range(peers)
            ]
            share = jnp.concatenate(share, axis=0)
            x = rows[chip].reshape(2 * count, width)
            gating = lax.dot_general(
                x, gate_ref[pl.ds(2 * n, 2)].reshape(2 * units, width),
                (((1,), (1,)), ((), ())), preferred_element_type=f32,
            )
            upward = lax.dot_general(
                x, up_ref[pl.ds(2 * n, 2)].reshape(2 * units, width),
                (((1,), (1,)), ((), ())), preferred_element_type=f32,
            )
            at = pl.ds(pl.multiple_of(n * 2 * units, 2 * units), 2 * units)
            hid[:, at] = (gating / (1.0 + jnp.exp(-gating)) * upward * share).astype(bf16)
            return carry

        lax.fori_loop(0, experts // 2, expert_pair, 0)

        def columns(n, carry):
            at = pl.ds(pl.multiple_of(n * 512, 512), 512)
            down = down_ref[:, :, at].reshape(experts * units, 512)
            made = jnp.dot(hid[...], down, preferred_element_type=f32)
            res[chip, :, :, :, at] = made.astype(bf16).reshape(2, peers, slots, 512)
            return carry

        lax.fori_loop(0, width // 512, columns, 0)
        send(res.at[chip, 1 - core], theirs.at[chip], pair_s.at[chip], pair_r.at[chip], other)

    def give_back(chip):
        arrived(theirs.at[chip], pair_s.at[chip], pair_r.at[chip])
        res[chip, core] = (res[chip, core].astype(f32) + theirs[chip].astype(f32)).astype(bf16)
        for j in (3, 1, 2):
            target = lax.rem(e + j, peers)
            send(
                res.at[chip, core, target], back.at[chip, e],
                back_s.at[chip, j], back_r.at[chip, j], (target, t),
            )
        back[chip, e] = res[chip, core, e]

    def unselect(chip):
        for j in range(1, peers):
            arrived(back.at[chip, sources[j]], back_s.at[chip, j], back_r.at[chip, j])
        for h in range(pieces):
            acc[chip, h] = lax.dot_general(
                spreads[chip],
                back[chip, :, :, h * part : (h + 1) * part].reshape(count, part),
                (((0,), (0,)), ((), ())), preferred_element_type=f32,
            ).astype(bf16)

    def add_from(total, piece, send_sem, recv_sem):
        @pl.when(inner)
        def _():
            arrived(piece, send_sem, recv_sem)
            total[...] = (total[...].astype(f32) + piece[...].astype(f32)).astype(bf16)

    def forward(chip, joins, which, when=None):
        device = at_chip(z + step + near_end * (chip - z - step))
        slot = chip + (near_end * (chips - chip) if joins else 0)
        for h in which:
            if joins:
                add_from(acc.at[chip, h], inb.at[chip, h], rs_s.at[chip, h], rs_r.at[chip, h])
            send(
                acc.at[chip, h], inb.at[slot, h], rs_s.at[chip, h], rs_r.at[slot, h], device, when
            )

    def keep_order():
        def body(i, carry):
            state[0] = jnp.zeros_like(state[0])
            return carry

        lax.fori_loop(0, t // (4 * chips), body, 0)

    written = []

    def finish(first, parts, sems, out, target, at):
        total = first[...].astype(f32)
        for piece, sem in zip(parts, sems[1:]):
            arrived(piece, sems[0], sem)
            total = total + piece[...].astype(f32)
        out[...] = total.astype(bf16)
        copy = pltpu.make_async_copy(out, target.at[:, at], out_sems.at[len(written)])
        copy.start()
        written.append(copy)

    heads = local.shape[0]

    def send_states():
        for j in range(1, peers):
            send(states_out, states_in.at[j], st_s.at[j], st_r.at[j], at_peer(j), e < peers - j)

    def project():
        state[...] = jnp.zeros_like(state)
        for j in range(peers - 1, 0, -1):
            @pl.when(e >= j)
            def _():
                arrived(states_in.at[j], st_s.at[j], st_r.at[j])
                for h in range(heads):
                    piece = states_in[j, h].astype(f32)
                    state[h] = piece[:, :DV] + mm(piece[:, DV:], state[h])
        for h in range(heads):
            attn[:, h * DV : (h + 1) * DV] = (local[h] + mm(proj[h], state[h])).astype(bf16)
        loads[15].wait()
        share = prod.shape[2]

        def columns(n, carry):
            at = pl.ds(pl.multiple_of(n * 512, 512), 512)
            made = jnp.dot(attn[...], wout_ref[:, at], preferred_element_type=f32)
            made = made.astype(bf16).reshape(chips, 2, share, 512)
            for c in range(2):
                prod[c, :, :, at] = made[:, c]
            return carry

        lax.fori_loop(0, width // 512, columns, 0)
        send(prod.at[1 - core], prod_theirs, pp_s, pp_r, other)

    def join_mixed():
        arrived(prod_theirs, pp_s, pp_r)
        prod[core] = (prod[core].astype(f32) + prod_theirs[...].astype(f32)).astype(bf16)

    def send_mixed(chip, slot, target, when):
        send(
            prod.at[core, chip], mixed_in.at[slot],
            mr_s.at[chip], mr_r.at[slot], at_chip(target), when,
        )

    def start_mixed():
        for n in (3, 2, 1):
            send_mixed(z + n * step, z + n * step, z + step, outer)
        send_mixed(z - step, z - step, z - step, inner)

    def pass_mixed():
        for n in (2, 1):
            chip = z + n * step

            @pl.when(inner)
            def _():
                arrived(mixed_in.at[chip], mr_s.at[chip], mr_r.at[chip])
                prod[core, chip] = (
                    prod[core, chip].astype(f32) + mixed_in[chip].astype(f32)
                ).astype(bf16)

            send_mixed(chip, chips, chip, inner)

    select(order(0))
    keep_order()
    for copy in loads[5:12]:
        copy.wait()
    strength_ref[...] = 1.0 / (1.0 + jnp.exp(-logit_ref[...].astype(f32)))
    before = before_ref[...].astype(f32)
    growth = jnp.maximum(before, 0.0) + jnp.log1p(jnp.exp(-jnp.abs(before)))
    for h in range(heads):
        decay_ref[h : h + 1] = (
            -jnp.exp(rate_ref[:, h : h + 1]) * growth[h : h + 1] + extra_ref[h : h + 1]
        )
    delta = delta_body(q_ref, k_ref, v_ref, strength_ref, decay_ref, local, proj, states_out)
    next(delta)
    keep_order()
    gathered(order(1))
    share_rows(3, order(1), z - step, inner)
    share_rows(1, z, z + step, inner)
    select(order(1))
    keep_order()
    next(delta)
    keep_order()
    send_states()
    pass_on(order(0))
    keep_order()
    for copy in loads[12:15]:
        copy.wait()
    produce(order(0))
    keep_order()
    gathered(order(2))
    share_rows(0, z, z + 2 * step, inner)
    select(order(2))
    keep_order()
    pass_on(order(1))
    keep_order()
    produce(order(1))
    keep_order()
    gathered(order(3))
    select(order(3))
    keep_order()
    project()
    keep_order()
    pass_on(order(2))
    keep_order()
    produce(order(2))
    keep_order()
    join_mixed()
    start_mixed()
    keep_order()
    give_back(returns[0])
    keep_order()
    pass_on(order(3))
    keep_order()
    produce(order(3))
    keep_order()
    give_back(returns[1])
    keep_order()
    give_back(returns[2])
    keep_order()
    give_back(order(0))
    keep_order()
    pass_mixed()
    keep_order()
    unselect(returns[0])
    keep_order()
    forward(returns[0], True, range(pieces))
    keep_order()
    unselect(returns[1])
    keep_order()
    forward(returns[1], False, range(pieces), outer)
    forward(returns[1], True, range(pieces // 2), inner)
    keep_order()
    finish(
        prod.at[core, z], (mixed_in.at[z], mixed_in.at[chips]),
        (mr_s.at[0], mr_r.at[z], mr_r.at[chips]), mixed_ref, mixed_hbm, pl.ds(0, width),
    )
    unselect(returns[2])
    keep_order()
    forward(returns[2], False, range(pieces))
    forward(returns[1], True, range(pieces // 2, pieces), inner)
    keep_order()
    unselect(order(0))
    keep_order()
    for h in range(pieces):
        finish(
            acc.at[z, h], (inb.at[z, h], inb.at[chips, h]),
            (rs_s.at[0, h], rs_r.at[z, h], rs_r.at[chips, h]),
            expert_ref.at[h], expert_hbm, pl.ds(h * part, part),
        )
    for copy in written:
        copy.wait()
    for make, when in started:
        if when is None:
            make().wait_send()
        else:
            @pl.when(when)
            def _():
                make().wait_send()


def hand_over_kernel(first, second, first_out, second_out, held, in_sems, out_sems):
    block = held.shape[1]
    moves = []
    for source, target in ((first, first_out), (second, second_out)):
        for n in range(source.shape[0] // block):
            at = pl.ds(n * block, block)
            i = len(moves)
            read = pltpu.make_async_copy(source.at[at], held.at[i], in_sems.at[i])
            write = pltpu.make_async_copy(held.at[i], target.at[at], out_sems.at[i])
            read.start()
            moves.append((read, write))
    for read, write in moves:
        read.wait()
        write.start()
    for read, write in moves:
        write.wait()


def hand_over(first, second):
    block = first.shape[0] // 2
    count = (first.shape[0] + second.shape[0]) // block
    anywhere = pl.BlockSpec(memory_space=pl.ANY)
    return pl.pallas_call(
        hand_over_kernel,
        out_shape=tuple(jax.ShapeDtypeStruct(a.shape, a.dtype) for a in (first, second)),
        in_specs=[anywhere] * 2,
        out_specs=(anywhere, anywhere),
        scratch_shapes=[
            pltpu.VMEM((count, block, first.shape[1]), first.dtype),
            pltpu.SemaphoreType.DMA((count,)),
            pltpu.SemaphoreType.DMA((count,)),
        ],
        compiler_params=pltpu.CompilerParams(vmem_limit_bytes=67043328),
    )(first, second)


def fused(
    tokens, scale, choice, router, difference, logit, before, rate, extra,
    queries, keys, values, gate, up, down, out_weight, slots,
):
    experts, units, width = gate.shape
    count, peers, chips, pieces = tokens.shape[0], lax.axis_size("ep"), RING, 4
    heads, length = extra.shape
    part = width // pieces
    share = length // (2 * chips)
    bf16, f32 = jnp.bfloat16, jnp.float32
    anywhere = pl.BlockSpec(memory_space=pl.ANY)
    dma = pltpu.SemaphoreType.DMA

    def room(*shape, dtype=bf16):
        return pltpu.VMEM(shape, dtype)

    arguments = [
        tokens, scale, choice, router, difference, logit, before, rate, extra,
        queries, keys, values, gate, up, down, out_weight,
    ]
    mixed, expert = pl.pallas_call(
        fused_kernel,
        out_shape=(
            jax.ShapeDtypeStruct((share, width), bf16),
            jax.ShapeDtypeStruct((count, width), bf16),
        ),
        in_specs=[anywhere] * len(arguments),
        out_specs=(anywhere, anywhere),
        scratch_shapes=[room(*a.shape, dtype=a.dtype) for a in arguments]
        + [
            room(chips, count, width),
            room(chips, (peers + 1) * 8, count, dtype=f32),
            room(chips, peers * slots, count),
            room(chips, peers, slots, width),
            room(chips, peers, 16, count),
            room(chips, 2, peers, slots, width),
            room(chips, 2, peers, 16, count),
            room(2 * peers * slots, experts * units),
            room(chips, 2, peers, slots, width),
            room(chips, peers, slots, width),
            room(chips, peers, slots, width),
            room(chips, pieces, count, part),
            room(chips + 1, pieces, count, part),
            room(heads, length, DV, dtype=f32),
            room(heads, length, DK, dtype=f32),
            room(length, heads * DV),
            room(heads, DK, DV + DK),
            room(peers, heads, DK, DV + DK),
            room(heads, DK, DV, dtype=f32),
            room(2, chips, share, width),
            room(chips, share, width),
            room(chips + 1, share, width),
            room(heads, length, dtype=f32),
            room(heads, length, dtype=f32),
            room(share, width),
            room(pieces, count, part),
            dma((len(arguments),)), dma((1 + pieces,)),
            dma((5,)), dma((chips,)), dma((5,)), dma((chips,)),
            dma((chips, peers)), dma((chips, peers)), dma((chips, peers)), dma((chips, peers)),
            dma((chips,)), dma((chips,)), dma((chips,)), dma((chips,)),
            dma((chips,)), dma((chips,)),
            dma((chips, peers)), dma((chips, peers)),
            dma((chips, pieces)), dma((chips + 1, pieces)),
            dma((peers,)), dma((peers,)), dma, dma,
            dma((chips,)), dma((chips + 1,)),
        ],
        cost_estimate=pl.CostEstimate(
            flops=12 * chips * peers * slots * experts * units * width,
            bytes_accessed=8 * experts * units * width,
            transcendentals=0,
        ),
        compiler_params=pltpu.CompilerParams(
            collective_id=0, has_side_effects=True, vmem_limit_bytes=63 * 2**20
        ),
    )(*arguments)
    return hand_over(mixed, expert)


def by_tokens(normed, choice, mixing, gate, up, down, slots, after):
    ep_count = lax.axis_size("ep")
    local_experts = gate.shape[0]
    tokens, width = normed.shape
    bf16 = jnp.bfloat16
    f32 = jnp.float32
    named = choice[:, :, None] == jnp.arange(ep_count * local_experts, dtype=jnp.int32)
    share = jnp.sum(jnp.where(named, mixing[:, :, None], 0.0), axis=1)
    goes = jnp.any(named, axis=1).reshape(tokens, ep_count, local_experts).any(axis=-1)
    earlier = jnp.tril(jnp.ones((tokens, tokens), bf16), -1)
    rank = jnp.dot(earlier, goes.astype(bf16), preferred_element_type=f32)
    spread = goes[:, :, None] & (rank[:, :, None] == jnp.arange(slots, dtype=f32))
    spread = spread.astype(bf16)
    high = share.astype(bf16)
    low = (share - high.astype(f32)).astype(bf16)
    sent = jnp.einsum("tes,td->esd", spread, normed, preferred_element_type=f32).astype(bf16)
    extra = jnp.concatenate(
        [
            high.reshape(tokens, ep_count, local_experts),
            low.reshape(tokens, ep_count, local_experts),
        ],
        axis=-1,
    )
    extra = jnp.einsum("tes,tex->esx", spread, extra, preferred_element_type=f32).astype(bf16)
    pad = -extra.shape[-1] % 128
    extra = jnp.pad(extra, ((0, 0), (0, 0), (0, pad)))
    outgoing = jnp.concatenate([sent, extra], axis=-1)
    arrived = lax.all_to_all(outgoing, "ep", split_axis=0, concat_axis=0, tiled=True)
    arrived = arrived.reshape(ep_count * slots, -1)
    everyone = lax.all_gather(arrived, "tp", axis=0, tiled=True)
    produced = expert_layer(everyone, gate, up, down, arrived.shape[0])
    summed = lax.psum_scatter(produced, "tp", scatter_dimension=0, tiled=True)
    returned = lax.all_to_all(
        summed.reshape(ep_count, slots, width), "ep", split_axis=0, concat_axis=0, tiled=True
    )
    combined = jnp.einsum("tes,esd->td", spread, returned, preferred_element_type=f32)
    return combined.astype(bf16), after


def by_weights(normed, expert_choice_index, mixing, gate, up, down):
    own_tokens, width_model = normed.shape
    ep_count = lax.axis_size("ep")
    local_experts = gate.shape[0]
    experts = local_experts * ep_count
    flat_ids = expert_choice_index.reshape(-1)
    one_hot = (flat_ids[:, None] == jnp.arange(experts, dtype=jnp.int32)[None, :]).astype(jnp.int32)
    slot_rank = jnp.sum((jnp.cumsum(one_hot, axis=0) - one_hot) * one_hot, axis=1)
    slot_index = flat_ids * CAP + slot_rank
    copy_token = jnp.arange(flat_ids.shape[0], dtype=jnp.int32) // TOPK
    slot_token = jnp.full((experts * CAP,), own_tokens, jnp.int32).at[slot_index].set(copy_token)
    outgoing = jnp.take(normed, slot_token, axis=0, mode="fill", fill_value=0).reshape(
        ep_count, local_experts, CAP, width_model
    )
    arrived = lax.all_to_all(outgoing, "ep", split_axis=0, concat_axis=0, tiled=True)
    gate_piece = lax.all_gather(gate, "tp", axis=1, tiled=True)
    up_piece = lax.all_gather(up, "tp", axis=1, tiled=True)
    down_piece = lax.all_gather(down, "tp", axis=1, tiled=True)
    gating = jnp.einsum("secd,efd->secf", arrived, gate_piece, preferred_element_type=jnp.float32)
    upward = jnp.einsum("secd,efd->secf", arrived, up_piece, preferred_element_type=jnp.float32)
    hidden = (jax.nn.silu(gating) * upward).astype(jnp.bfloat16)
    produced = jnp.einsum("secf,efd->secd", hidden, down_piece, preferred_element_type=jnp.float32)
    returned = lax.all_to_all(
        produced.astype(jnp.bfloat16), "ep", split_axis=0, concat_axis=0, tiled=True
    )
    flat_results = returned.reshape(experts * CAP, width_model)
    picked = (
        jnp.take(flat_results, slot_index, axis=0)
        .reshape(own_tokens, TOPK, width_model)
        .astype(jnp.float32)
    )
    return jnp.sum(mixing[..., None] * picked, axis=1).astype(jnp.bfloat16)


def shards(
    query_heads_rows,
    key_heads_rows,
    value_heads_rows,
    write_strength_logit,
    decay_preactivation,
    head_decay_logarithm,
    extra_log_decay,
    output_weight,
    second_batch_tokens,
    expert_norm_scale,
    expert_choice_index,
    group_router_weight,
    expert_logit_difference,
    expert_gate_weight,
    expert_up_weight,
    expert_down_weight,
):
    length = query_heads_rows.shape[0]
    local_heads = head_decay_logarithm.shape[0]
    strength = jax.nn.sigmoid(write_strength_logit.astype(jnp.float32))
    decay_logarithm = (
        -jnp.exp(head_decay_logarithm)[:, None]
        * jax.nn.softplus(decay_preactivation.astype(jnp.float32))
        + extra_log_decay
    )
    leading = jax.nn.sigmoid(expert_logit_difference)
    mixing = group_router_weight[:, None] * jnp.stack([leading, 1.0 - leading], axis=-1)
    local_experts, local_units, width = expert_gate_weight.shape
    own_tokens = second_batch_tokens.shape[0]
    ep_count, tp_count = lax.axis_size("ep"), lax.axis_size("tp")
    named_both = TOPK if local_experts % EPG == 0 else 1
    slots = min(own_tokens, local_experts * CAP // named_both)
    weights = (expert_gate_weight, expert_up_weight, expert_down_weight)
    if (
        (ep_count, tp_count) == (RING, 2 * RING)
        and named_both == TOPK
        and own_tokens == DK
        and local_experts * local_units == width // RING
    ):
        return fused(
            second_batch_tokens, expert_norm_scale.reshape(1, width), expert_choice_index.T,
            group_router_weight.reshape(1, own_tokens),
            expert_logit_difference.reshape(1, own_tokens),
            write_strength_logit, decay_preactivation,
            head_decay_logarithm.reshape(1, local_heads), extra_log_decay,
            query_heads_rows, key_heads_rows, value_heads_rows, *weights, output_weight, slots,
        )
    local_output, projection_matrix, end_memory = delta_rule(
        query_heads_rows, key_heads_rows, value_heads_rows, strength, decay_logarithm
    )
    incoming_rows = incoming(end_memory, "ep")
    attention_result = local_output + jnp.einsum(
        "hpg,hgd->hpd", projection_matrix, incoming_rows, precision=precise_setting
    )
    attn_rows = (
        attention_result.transpose(1, 0, 2)
        .reshape(length, local_heads * DV)
        .astype(jnp.bfloat16)
    )
    product = jnp.dot(attn_rows, output_weight, preferred_element_type=jnp.float32)
    product = product.astype(jnp.bfloat16)
    widened = second_batch_tokens.astype(jnp.float32)
    normed = (
        widened
        * lax.rsqrt(jnp.mean(widened * widened, axis=-1, keepdims=True) + norm_eps)
        * expert_norm_scale
    ).astype(jnp.bfloat16)
    if 2 * tp_count * ep_count * slots < 3 * local_experts * local_units * tp_count:
        expert_out, product = by_tokens(
            normed, expert_choice_index, mixing, *weights, slots, product
        )
    else:
        expert_out = by_weights(normed, expert_choice_index, mixing, *weights)
    summed = lax.psum_scatter(product, "tp", scatter_dimension=0, tiled=True)
    return (summed, expert_out)


def solution(mesh):
    in_specs = (
        P("ep", "tp"),
        P("ep", "tp"),
        P("ep", "tp"),
        P("tp", "ep"),
        P("tp", "ep"),
        P("tp"),
        P("tp", "ep"),
        P("tp", None),
        P(("ep", "tp"), None),
        P(),
        P(("ep", "tp"), None),
        P(("ep", "tp")),
        P(("ep", "tp")),
        P("ep", "tp", None),
        P("ep", "tp", None),
        P("ep", "tp", None),
    )
    out_specs = (P(("ep", "tp"), None), P(("ep", "tp"), None))
    return jax.shard_map(shards, mesh=mesh, in_specs=in_specs, out_specs=out_specs, check_vma=False)
```
